512 devices in a mesh: sp: 16 (over y, x), tp: 32 (over z, core).
Axes of the slice: x: 4, y: 4, z: 16, core: 2. Of those that a mesh axis runs over, the one named last changes fastest.
Arguments:
- stream: bfloat16 [8192, 4096], P('sp', 'tp'), may hold values from -6 to 6
- gain_first: bfloat16 [4096], P('tp'), may hold values from 0.099609375 to 1.8984375
- query_first: bfloat16 [4096, 4096], P('sp', 'tp'), may hold values from -0.09375 to 0.09375
- key_first: bfloat16 [4096, 4096], P('sp', 'tp'), may hold values from -0.09375 to 0.09375
- value_first: bfloat16 [4096, 4096], P('sp', 'tp'), may hold values from -0.09375 to 0.09375
- offset_first: float32 [32, 15, 31], P('tp'), may hold values from -4 to 254
- gain_second: bfloat16 [4096], P('tp'), may hold values from 0.099609375 to 1.8984375
- query_second: bfloat16 [4096, 4096], P('sp', 'tp'), may hold values from -0.09375 to 0.09375
- key_second: bfloat16 [4096, 4096], P('sp', 'tp'), may hold values from -0.09375 to 0.09375
- value_second: bfloat16 [4096, 4096], P('sp', 'tp'), may hold values from -0.09375 to 0.09375
- offset_second: float32 [32, 15, 31], P('tp'), may hold values from -4 to 254
Outputs:
- result: bfloat16 [8192, 4096], P('sp', 'tp')
The draws below stay inside these ranges and needn't reach their ends.
All inputs are finite; a program needn't handle non-finite values.
Results may differ from the reference program's by a relative error of at most 0.008.
Values may be sent and summed in bfloat16 or wider, within the bound.
No kernel may reach another device: no remote copies, remote signals or barrier semaphores. Data moves between devices by JAX's collectives and lax.ppermute only.
A program may use at most 64 MiB of HBM per device.

```python
import jax
import jax.numpy as jnp
import numpy as np
from jax import lax

GRID_W = 64
HEAD_DIM = 128
HEADS = 32
D = 4096
TOKENS = 8192


def draw_stream(key, part):
    first, second = jax.random.split(jax.random.fold_in(key, 11))
    blocks = D // HEAD_DIM
    scales = jnp.exp(jax.random.uniform(first, (blocks,), jnp.float32, jnp.log(0.15), jnp.log(1.0)))
    base = jnp.clip(jax.random.normal(second, (TOKENS, D), jnp.float32), -6.0, 6.0)
    return (base * jnp.repeat(scales, HEAD_DIM)[None, :]).astype(jnp.bfloat16)


def draw_table(key):
    base = jnp.clip(jax.random.normal(key, (HEADS, 15, 31), jnp.float32), -4.0, 4.0)
    return base


def draw_offset_first(key, part):
    return draw_table(jax.random.fold_in(key, 21))


def draw_offset_second(key, part):
    return draw_table(jax.random.fold_in(key, 22))


def levels(key, dims, cuts, least, high):
    level = 1.0
    for axis_at, blocks in cuts:
        steps = jax.random.uniform(jax.random.fold_in(jax.random.fold_in(key, 6), axis_at), (blocks,), jnp.float32, least / len(cuts), high / len(cuts))
        level = level * jnp.repeat(jnp.exp(steps), dims[axis_at] // blocks).reshape((-1,) + (1,) * (len(dims) - 1 - axis_at))
    return level


def normal_values(key, shape, scale, bound, cuts=(), held_as=jnp.bfloat16):
    factor_of = levels(key, shape, cuts, -0.22, 0.18) if cuts else 1.0
    values = jax.random.normal(key, shape, jnp.float32) * scale * factor_of
    return jnp.minimum(jnp.maximum(values, -bound), bound).astype(held_as)


def setup_inputs(seed: int = 0) -> dict:
    key_of = jax.random.split(jax.random.key(seed), 12)
    stream = draw_stream(jax.random.fold_in(key_of[11], 71), 0)
    gain_first = jnp.clip(1.0 + 0.18 * jax.random.normal(key_of[1], (D,), jnp.float32), 0.099609375, 1.8984375).astype(jnp.bfloat16)
    query_first = normal_values(key_of[2], (D, D), D ** -0.5, 0.09375, ((0, 16), (1, 32)))
    key_first = normal_values(key_of[3], (D, D), D ** -0.5, 0.09375, ((0, 16), (1, 32)))
    value_first = normal_values(key_of[4], (D, D), D ** -0.5, 0.09375, ((0, 16), (1, 32)))
    offset_first = draw_offset_first(jax.random.fold_in(key_of[11], 71), 0)
    gain_second = jnp.clip(1.0 + 0.18 * jax.random.normal(key_of[6], (D,), jnp.float32), 0.099609375, 1.8984375).astype(jnp.bfloat16)
    query_second = normal_values(key_of[7], (D, D), D ** -0.5, 0.09375, ((0, 16), (1, 32)))
    key_second = normal_values(key_of[8], (D, D), D ** -0.5, 0.09375, ((0, 16), (1, 32)))
    value_second = normal_values(key_of[9], (D, D), D ** -0.5, 0.09375, ((0, 16), (1, 32)))
    offset_second = draw_offset_second(jax.random.fold_in(key_of[11], 71), 0)
    return {"stream": stream, "gain_first": gain_first, "query_first": query_first, "key_first": key_first, "value_first": value_first, "offset_first": offset_first, "gain_second": gain_second, "query_second": query_second, "key_second": key_second, "value_second": value_second, "offset_second": offset_second}


epsilon = 1e-06

def normalize(stream, gain):
    widened = stream.astype(jnp.float32)
    mean_square = lax.optimization_barrier(jnp.mean(widened * widened, axis=-1, keepdims=True))
    return (widened * lax.rsqrt(mean_square + epsilon) * gain.astype(jnp.float32)).astype(jnp.bfloat16)

def attend(query, keys, values, table, row_start, total_rows):
    rows_here, width, heads, head_size = query.shape
    blocks = width // 16
    query_cols = np.arange(width).reshape(blocks, 16)
    window_start = np.clip(query_cols - 8, 0, width - 16)
    key_cols = np.clip(np.arange(blocks) * 16 - 8, 0, width - 32)[:, None] + np.arange(32)
    column_ok = (key_cols[:, None, :] >= window_start[:, :, None]) & (key_cols[:, None, :] < window_start[:, :, None] + 16)
    column_offset = np.clip(key_cols[:, None, :] - query_cols[:, :, None] + 15, 0, 30)
    column_bias = table.astype(jnp.float32)[:, :, column_offset]
    mask = jnp.asarray(column_ok)[None, :, :, None, :]
    factor = head_size ** (-0.5)

    def one_row(index):
        grid_row = row_start + index
        first = jnp.clip(grid_row - 4, 0, total_rows - 8)
        local = first - row_start + 4
        key_block = lax.dynamic_slice_in_dim(keys, local, 8, 0)[:, key_cols].astype(jnp.float32)
        value_block = lax.dynamic_slice_in_dim(values, local, 8, 0)[:, key_cols].astype(jnp.float32)
        query_row = lax.dynamic_index_in_dim(query, index, 0, keepdims=False).reshape(blocks, 16, heads, head_size)
        scores = jnp.einsum('jqhe,mjkhe->hjqmk', query_row.astype(jnp.float32), key_block) * factor
        row_offset = first + jnp.arange(8, dtype=jnp.int32) - grid_row + 7
        row_bias = jnp.transpose(jnp.take(column_bias, row_offset, axis=1), (0, 2, 3, 1, 4))
        scores = jnp.where(mask, scores + row_bias, -1e+30)
        weight = jax.nn.softmax(scores.reshape(heads, blocks, 16, 256), axis=-1)
        rounded = weight.astype(jnp.bfloat16).reshape(heads, blocks, 16, 8, 32)
        output = jnp.einsum('hjqmk,mjkhe->jqhe', rounded.astype(jnp.float32), value_block)
        return output.reshape(width, heads * head_size)
    return lax.map(one_row, jnp.arange(rows_here, dtype=jnp.int32))

def layer(stream, gain, w_query, w_key, w_value, table):
    normed = normalize(stream, gain)
    query = jnp.dot(normed, w_query, preferred_element_type=jnp.float32).astype(jnp.bfloat16)
    keys = jnp.dot(normed, w_key, preferred_element_type=jnp.float32).astype(jnp.bfloat16)
    values = jnp.dot(normed, w_value, preferred_element_type=jnp.float32).astype(jnp.bfloat16)
    total_rows = stream.shape[0] // GRID_W
    shape = (total_rows, GRID_W, HEADS, HEAD_DIM)
    padding = ((4, 4), (0, 0), (0, 0), (0, 0))
    keys = jnp.pad(keys.reshape(shape), padding)
    values = jnp.pad(values.reshape(shape), padding)
    output = attend(query.reshape(shape), keys, values, table, 0, total_rows)
    return (stream.astype(jnp.float32) + output.reshape(stream.shape)).astype(jnp.bfloat16)

def reference(stream, gain_first, query_first, key_first, value_first, offset_first, gain_second, query_second, key_second, value_second, offset_second):
    middle = layer(stream, gain_first, query_first, key_first, value_first, offset_first)
    return layer(middle, gain_second, query_second, key_second, value_second, offset_second)
```

```python
import functools

import jax
import jax.numpy as jnp
import numpy as np
from jax import lax
from jax.experimental import pallas as pl
from jax.experimental.pallas import tpu as pltpu
from jax.sharding import PartitionSpec as P

GRID_W = 64
EPSILON = 1e-06
SCALE_FIRST = 2.0**13
SCALE_SECOND = 2.0**6
WINDOW_ROWS = 8
HALO = 4
MASKED = -1e30


def vmem():
    return pl.BlockSpec(memory_space=pltpu.VMEM)


def bias_kernel(first_ref, second_ref, first_out, second_out):
    width = GRID_W
    col = lax.broadcasted_iota(jnp.int32, (width, 2 * width), 0)
    key = lax.broadcasted_iota(jnp.int32, (width, 2 * width), 1) % width
    start = jnp.clip(col - 8, 0, width - 16)
    inside = (key >= start) & (key < start + 16)
    for table_ref, out_ref in ((first_ref, first_out), (second_ref, second_out)):
        table = table_ref[0]
        low = jnp.pad(table, ((0, 1), (0, 2 * width - 31)))
        both = low + pltpu.roll(pltpu.roll(low, 15, 0), width, 1)
        for m in range(14):
            row = jnp.broadcast_to(both[m : m + 1, :], (width, 2 * width))
            turned = pltpu.roll(row, 2 * width - 15, 1, stride=1, stride_axis=0)
            out_ref[m] = jnp.where(inside, turned, MASKED)


def biases(first, second):
    shape = jax.ShapeDtypeStruct((14, GRID_W, 2 * GRID_W), jnp.float32)
    return pl.pallas_call(
        bias_kernel,
        out_shape=(shape, shape),
        in_specs=[vmem(), vmem()],
        out_specs=(vmem(), vmem()),
        name="biases",
    )(first, second)


def project_kernel(x_ref, gain_ref, w_ref, q_ref, k_ref, v_ref, normed):
    blocks, tokens, size = x_ref.shape
    total = jnp.zeros((tokens, size), jnp.float32)
    for f in range(blocks):
        part = x_ref[f].astype(jnp.float32)
        total = total + part * part
    mean = jnp.sum(total, axis=1, keepdims=True) * (1.0 / (blocks * size))
    rate = lax.rsqrt(mean + EPSILON)
    for f in range(blocks):
        part = x_ref[f].astype(jnp.float32)
        gain = gain_ref[f : f + 1, :].astype(jnp.float32)
        normed[:, f * size : (f + 1) * size] = (part * rate * gain).astype(jnp.bfloat16)
    half = tokens // 2
    for t in range(2):
        rows = slice(t * half, (t + 1) * half)
        out = jnp.dot(normed[rows, :], w_ref[...], preferred_element_type=jnp.float32)
        out = out.astype(jnp.bfloat16)
        q_ref[rows, :] = out[:, :size]
        k_ref[rows, :] = out[:, size : 2 * size]
        v_ref[rows, :] = out[:, 2 * size :]


def project(x, gain, weights):
    blocks, tokens, size = x.shape
    shape = jax.ShapeDtypeStruct((tokens, size), jnp.bfloat16)
    return pl.pallas_call(
        project_kernel,
        out_shape=(shape,) * 3,
        in_specs=[vmem()] * 3,
        out_specs=(vmem(),) * 3,
        scratch_shapes=[pltpu.VMEM((tokens, blocks * size), jnp.bfloat16)],
        cost_estimate=pl.CostEstimate(
            flops=2 * tokens * blocks * size * 3 * size, bytes_accessed=8 << 20, transcendentals=0
        ),
        name="project",
    )(x, gain, weights)


def attend_kernel(at_ref, q_ref, k_ref, v_ref, klo_ref, khi_ref, vlo_ref, vhi_ref, bias_ref, x_ref, out_ref, keys, values):
    width = GRID_W
    tokens, size = q_ref.shape
    rows = tokens // width
    edge = HALO * width
    keys[:edge] = klo_ref[...]
    keys[edge : edge + tokens] = k_ref[...]
    keys[edge + tokens :] = khi_ref[...]
    values[:edge] = vlo_ref[...]
    values[edge : edge + tokens] = v_ref[...]
    values[edge + tokens :] = vhi_ref[...]
    row_start, last = at_ref[0], at_ref[1]
    factor = size ** (-0.5)
    for r in range(rows):
        grid_row = row_start + r
        first = jnp.clip(grid_row - HALO, 0, last)
        at = pl.multiple_of((first - row_start + HALO) * width, width)
        offset = first - grid_row + 7
        span = pl.ds(at, WINDOW_ROWS * width)
        query = q_ref[r * width : (r + 1) * width, :]
        scores = lax.dot_general(
            query, keys[span, :], (((1,), (1,)), ((), ())), preferred_element_type=jnp.float32
        )
        parts = [
            scores[:, 2 * p * width : 2 * (p + 1) * width] * factor + bias_ref[offset + 2 * p]
            for p in range(WINDOW_ROWS // 2)
        ]
        top = functools.reduce(jnp.maximum, parts)
        top = jnp.max(top, axis=1, keepdims=True)
        parts = [jnp.exp(part - top) for part in parts]
        total = jnp.sum(functools.reduce(jnp.add, parts), axis=1, keepdims=True)
        weight = jnp.concatenate([(part / total).astype(jnp.bfloat16) for part in parts], axis=1)
        attended = jnp.dot(weight, values[span, :], preferred_element_type=jnp.float32)
        here = slice(r * width, (r + 1) * width)
        out_ref[here, :] = (x_ref[here, :].astype(jnp.float32) + attended).astype(jnp.bfloat16)


def attend(at, query, key, value, low, high, bias, x):
    tokens, size = query.shape
    long = tokens + 2 * HALO * GRID_W
    return pl.pallas_call(
        attend_kernel,
        out_shape=jax.ShapeDtypeStruct((tokens, size), jnp.bfloat16),
        in_specs=[pl.BlockSpec(memory_space=pltpu.SMEM)] + [vmem()] * 9,
        out_specs=vmem(),
        scratch_shapes=[pltpu.VMEM((long, size), jnp.bfloat16)] * 2,
        cost_estimate=pl.CostEstimate(
            flops=4 * tokens * size * WINDOW_ROWS * GRID_W, bytes_accessed=2 << 20, transcendentals=tokens * 512
        ),
        name="attend",
    )(at, query, key, value, low[0], high[0], low[1], high[1], bias, x)


def layer(x, gathered, gain, weights, bias, at):
    query, key, value = project(gathered, gain, weights)
    count = lax.axis_size("sp")
    forward = [(i, i + 1) for i in range(count - 1)]
    backward = [(target, source) for source, target in forward]
    edge = HALO * GRID_W
    low = lax.ppermute(jnp.stack([key[-edge:], value[-edge:]]), "sp", forward)
    high = lax.ppermute(jnp.stack([key[:edge], value[:edge]]), "sp", backward)
    return attend(at, query, key, value, low, high, bias, x)


def body(
    stream,
    gain_first,
    query_first,
    key_first,
    value_first,
    offset_first,
    gain_second,
    query_second,
    key_second,
    value_second,
    offset_second,
):
    tokens, size = stream.shape
    rows = tokens // GRID_W
    first_set = lax.all_gather(
        jnp.concatenate([query_first, key_first, value_first], 1), "sp", axis=0, tiled=True
    )
    second_set = lax.all_gather(
        jnp.concatenate([query_second, key_second, value_second], 1), "sp", axis=0, tiled=True
    )
    bias_first, bias_second = biases(offset_first, offset_second)
    start = lax.axis_index("sp") * rows
    total_rows = rows * lax.axis_size("sp")
    at = jnp.stack([start, jnp.int32(total_rows - WINDOW_ROWS)]).astype(jnp.int32)

    gains = jnp.pad(jnp.stack([gain_first, gain_second]), ((0, 14), (0, 0)))
    sent = (jnp.concatenate([stream, gains]).astype(jnp.float32) * SCALE_FIRST).astype(jnp.float16)
    held = lax.all_gather(sent, "tp", axis=0, tiled=False)
    held = (held.astype(jnp.float32) * (1.0 / SCALE_FIRST)).astype(jnp.bfloat16)
    middle = layer(stream, held[:, :tokens], held[:, tokens], first_set, bias_first, at)

    sent = (middle.astype(jnp.float32) * SCALE_SECOND).astype(jnp.float16)
    again = lax.all_gather(sent, "tp", axis=0, tiled=False)
    again = (again.astype(jnp.float32) * (1.0 / SCALE_SECOND)).astype(jnp.bfloat16)
    return layer(middle, again, held[:, tokens + 1], second_set, bias_second, at)


def solution(mesh):
    placed = (
        P("sp", "tp"),
        P("tp"),
        P("sp", "tp"),
        P("sp", "tp"),
        P("sp", "tp"),
        P("tp", None, None),
        P("tp"),
        P("sp", "tp"),
        P("sp", "tp"),
        P("sp", "tp"),
        P("tp", None, None),
    )
    return jax.shard_map(body, mesh=mesh, in_specs=placed, out_specs=P("sp", "tp"), check_vma=False)
```

```python
import functools

import jax
import jax.numpy as jnp
import numpy as np
from jax import lax
from jax.experimental import pallas as pl
from jax.experimental.pallas import tpu as pltpu
from jax.sharding import PartitionSpec as P

GRID_W = 64
EPSILON = 1e-06
SCALE_FIRST = 2.0**13
SCALE_SECOND = 2.0**6
WINDOW_ROWS = 8
HALO = 4
MASKED = -1e30
PROJECT_VMEM = 24 << 20
ATTEND_VMEM = 12 << 20


def vmem():
    return pl.BlockSpec(memory_space=pltpu.VMEM)


def bias_kernel(first_ref, second_ref, first_out, second_out):
    width = GRID_W
    col = lax.broadcasted_iota(jnp.int32, (width, 2 * width), 0)
    key = lax.broadcasted_iota(jnp.int32, (width, 2 * width), 1) % width
    start = jnp.clip(col - 8, 0, width - 16)
    inside = (key >= start) & (key < start + 16)
    for table_ref, out_ref in ((first_ref, first_out), (second_ref, second_out)):
        table = table_ref[0]
        low = jnp.pad(table, ((0, 1), (0, 2 * width - 31)))
        both = low + pltpu.roll(pltpu.roll(low, 15, 0), width, 1)
        for m in range(14):
            row = jnp.broadcast_to(both[m : m + 1, :], (width, 2 * width))
            turned = pltpu.roll(row, 2 * width - 15, 1, stride=1, stride_axis=0)
            out_ref[m] = jnp.where(inside, turned, MASKED)


def biases(first, second):
    shape = jax.ShapeDtypeStruct((14, GRID_W, 2 * GRID_W), jnp.float32)
    return pl.pallas_call(
        bias_kernel,
        out_shape=(shape, shape),
        in_specs=[vmem(), vmem()],
        out_specs=(vmem(), vmem()),
        compiler_params=pltpu.CompilerParams(vmem_limit_bytes=ATTEND_VMEM),
        name="biases",
    )(first, second)


def project_kernel(half, gain_row, scale, x_ref, gain_ref, w_ref, q_ref, kv_ref, normed):
    blocks, _, size = x_ref.shape
    tokens = q_ref.shape[0]
    rows = slice(half * tokens, (half + 1) * tokens)
    total = jnp.zeros((tokens, size), jnp.float32)
    for f in range(blocks):
        part = x_ref[f, rows, :].astype(jnp.float32)
        total = total + part * part
    mean = jnp.sum(total, axis=1, keepdims=True) * (1.0 / (blocks * size * scale * scale))
    rate = lax.rsqrt(mean + EPSILON) * (1.0 / scale)
    for f in range(blocks):
        part = x_ref[f, rows, :].astype(jnp.float32)
        gain = gain_ref[f, gain_row : gain_row + 1, :].astype(jnp.float32) * (1.0 / SCALE_FIRST)
        normed[:, f * size : (f + 1) * size] = (part * rate * gain).astype(jnp.bfloat16)
    out = jnp.dot(normed[...], w_ref[...], preferred_element_type=jnp.float32).astype(jnp.bfloat16)
    q_ref[...] = out[:, :size]
    kv_ref[0] = out[:, size : 2 * size]
    kv_ref[1] = out[:, 2 * size :]


def project(half, gain_row, scale, x, gain, weights, tokens):
    blocks, _, size = x.shape
    part = tokens // 2
    return pl.pallas_call(
        functools.partial(project_kernel, half, gain_row, scale),
        out_shape=(
            jax.ShapeDtypeStruct((part, size), jnp.bfloat16),
            jax.ShapeDtypeStruct((2, part, size), jnp.bfloat16),
        ),
        in_specs=[vmem()] * 3,
        out_specs=(vmem(),) * 2,
        scratch_shapes=[pltpu.VMEM((part, blocks * size), jnp.bfloat16)],
        cost_estimate=pl.CostEstimate(
            flops=2 * part * blocks * size * 3 * size, bytes_accessed=8 << 20, transcendentals=0
        ),
        compiler_params=pltpu.CompilerParams(vmem_limit_bytes=PROJECT_VMEM),
        name="project",
    )(x, gain, weights)


def attend_kernel(at_ref, qa_ref, qb_ref, low_ref, a_ref, b_ref, high_ref, bias_ref, x_ref, out_ref, keys, values):
    width = GRID_W
    half, size = qa_ref.shape
    rows = 2 * half // width
    for i, ref in enumerate((low_ref, a_ref, b_ref, high_ref)):
        keys[i * half : (i + 1) * half] = ref[0]
        values[i * half : (i + 1) * half] = ref[1]
    row_start, last = at_ref[0], at_ref[1]
    factor = size ** (-0.5)
    for r in range(rows):
        grid_row = row_start + r
        first = jnp.clip(grid_row - HALO, 0, last)
        at = pl.multiple_of((first - row_start + HALO) * width, width)
        offset = first - grid_row + 7
        span = pl.ds(at, WINDOW_ROWS * width)
        source, inner = (qa_ref, r) if r < rows // 2 else (qb_ref, r - rows // 2)
        query = source[inner * width : (inner + 1) * width, :]
        scores = lax.dot_general(
            query, keys[span, :], (((1,), (1,)), ((), ())), preferred_element_type=jnp.float32
        )
        parts = [
            scores[:, 2 * p * width : 2 * (p + 1) * width] * factor + bias_ref[offset + 2 * p]
            for p in range(WINDOW_ROWS // 2)
        ]
        top = functools.reduce(jnp.maximum, parts)
        top = jnp.max(top, axis=1, keepdims=True)
        parts = [jnp.exp(part - top) for part in parts]
        total = jnp.sum(functools.reduce(jnp.add, parts), axis=1, keepdims=True)
        inverse = 1.0 / total
        weight = jnp.concatenate([(part * inverse).astype(jnp.bfloat16) for part in parts], axis=1)
        attended = jnp.dot(weight, values[span, :], preferred_element_type=jnp.float32)
        here = slice(r * width, (r + 1) * width)
        out_ref[here, :] = (x_ref[here, :].astype(jnp.float32) + attended).astype(jnp.bfloat16)


def attend(at, queries, low, own, high, bias, x):
    tokens, size = x.shape
    long = tokens + 2 * HALO * GRID_W
    return pl.pallas_call(
        attend_kernel,
        out_shape=jax.ShapeDtypeStruct((tokens, size), jnp.bfloat16),
        in_specs=[pl.BlockSpec(memory_space=pltpu.SMEM)] + [vmem()] * 8,
        out_specs=vmem(),
        scratch_shapes=[pltpu.VMEM((long, size), jnp.bfloat16)] * 2,
        cost_estimate=pl.CostEstimate(
            flops=4 * tokens * size * WINDOW_ROWS * GRID_W, bytes_accessed=2 << 20, transcendentals=tokens * 512
        ),
        compiler_params=pltpu.CompilerParams(vmem_limit_bytes=ATTEND_VMEM),
        name="attend",
    )(at, *queries, low, *own, high, bias, x)


def layer(x, gathered, gain_row, scale, gains, weights, bias, at):
    tokens = x.shape[0]
    count = lax.axis_size("sp")
    forward = [(i, i + 1) for i in range(count - 1)]
    backward = [(target, source) for source, target in forward]
    query_high, own_high = project(1, gain_row, scale, gathered, gains, weights, tokens)
    low = lax.ppermute(own_high, "sp", forward)
    query_low, own_low = project(0, gain_row, scale, gathered, gains, weights, tokens)
    high = lax.ppermute(own_low, "sp", backward)
    return attend(at, (query_low, query_high), low, (own_low, own_high), high, bias, x)


def body(
    stream,
    gain_first,
    query_first,
    key_first,
    value_first,
    offset_first,
    gain_second,
    query_second,
    key_second,
    value_second,
    offset_second,
):
    tokens, size = stream.shape
    rows = tokens // GRID_W
    first_set = lax.all_gather(
        jnp.concatenate([query_first, key_first, value_first], 1), "sp", axis=0, tiled=True
    )
    second_set = lax.all_gather(
        jnp.concatenate([query_second, key_second, value_second], 1), "sp", axis=0, tiled=True
    )
    bias_first, bias_second = biases(offset_first, offset_second)
    start = lax.axis_index("sp") * rows
    total_rows = rows * lax.axis_size("sp")
    at = jnp.stack([start, jnp.int32(total_rows - WINDOW_ROWS)]).astype(jnp.int32)

    gains = jnp.pad(jnp.stack([gain_first, gain_second]), ((0, 14), (0, 0)))
    sent = (jnp.concatenate([stream, gains]).astype(jnp.float32) * SCALE_FIRST).astype(jnp.float16)
    held = lax.all_gather(sent, "tp", axis=0, tiled=False).astype(jnp.bfloat16)
    gains = held[:, tokens:]
    middle = layer(stream, held, 0, SCALE_FIRST, gains, first_set, bias_first, at)
    sent = (middle.astype(jnp.float32) * SCALE_SECOND).astype(jnp.float16)
    again = lax.all_gather(sent, "tp", axis=0, tiled=False).astype(jnp.bfloat16)
    return layer(middle, again, 1, SCALE_SECOND, gains, second_set, bias_second, at)


def solution(mesh):
    placed = (
        P("sp", "tp"),
        P("tp"),
        P("sp", "tp"),
        P("sp", "tp"),
        P("sp", "tp"),
        P("tp", None, None),
        P("tp"),
        P("sp", "tp"),
        P("sp", "tp"),
        P("sp", "tp"),
        P("tp", None, None),
    )
    return jax.shard_map(body, mesh=mesh, in_specs=placed, out_specs=P("sp", "tp"), check_vma=False)
```

```python
import functools

import jax
import jax.numpy as jnp
import numpy as np
from jax import lax
from jax.experimental import pallas as pl
from jax.experimental.pallas import tpu as pltpu
from jax.sharding import PartitionSpec as P

GRID_W = 64
EPSILON = 1e-06
SCALE_FIRST = 2.0**13
SCALE_SECOND = 2.0**6
WINDOW_ROWS = 8
HALO = 4
MASKED = -1e30
PROJECT_VMEM = 24 << 20
ATTEND_VMEM = 12 << 20


def vmem():
    return pl.BlockSpec(memory_space=pltpu.VMEM)


def bias_kernel(first_ref, second_ref, first_out, second_out):
    width = GRID_W
    col = lax.broadcasted_iota(jnp.int32, (width, 2 * width), 0)
    key = lax.broadcasted_iota(jnp.int32, (width, 2 * width), 1) % width
    start = jnp.clip(col - 8, 0, width - 16)
    inside = (key >= start) & (key < start + 16)
    for table_ref, out_ref in ((first_ref, first_out), (second_ref, second_out)):
        table = table_ref[0]
        low = jnp.pad(table, ((0, 1), (0, 2 * width - 31)))
        both = low + pltpu.roll(pltpu.roll(low, 15, 0), width, 1)
        for m in range(14):
            row = jnp.broadcast_to(both[m : m + 1, :], (width, 2 * width))
            turned = pltpu.roll(row, 2 * width - 15, 1, stride=1, stride_axis=0)
            out_ref[m] = jnp.where(inside, turned, MASKED)


def biases(first, second):
    shape = jax.ShapeDtypeStruct((14, GRID_W, 2 * GRID_W), jnp.float32)
    return pl.pallas_call(
        bias_kernel,
        out_shape=(shape, shape),
        in_specs=[vmem(), vmem()],
        out_specs=(vmem(), vmem()),
        compiler_params=pltpu.CompilerParams(vmem_limit_bytes=ATTEND_VMEM),
        name="biases",
    )(first, second)


def project_kernel(half, gain_row, scale, x_ref, gain_ref, w_ref, q_ref, kv_ref, normed):
    blocks, _, size = x_ref.shape
    tokens = q_ref.shape[0]
    rows = slice(half * tokens, (half + 1) * tokens)
    total = jnp.zeros((tokens, size), jnp.float32)
    for f in range(blocks):
        part = x_ref[f, rows, :].astype(jnp.float32)
        total = total + part * part
    mean = jnp.sum(total, axis=1, keepdims=True) * (1.0 / (blocks * size * scale * scale))
    rate = lax.rsqrt(mean + EPSILON) * (1.0 / scale)
    for f in range(blocks):
        part = x_ref[f, rows, :].astype(jnp.float32)
        gain = gain_ref[f, gain_row : gain_row + 1, :].astype(jnp.float32) * (1.0 / SCALE_FIRST)
        normed[:, f * size : (f + 1) * size] = (part * rate * gain).astype(jnp.bfloat16)
    out = jnp.dot(normed[...], w_ref[...], preferred_element_type=jnp.float32).astype(jnp.bfloat16)
    q_ref[...] = out[:, :size]
    kv_ref[0] = out[:, size : 2 * size]
    kv_ref[1] = out[:, 2 * size :]


def project(half, gain_row, scale, x, gain, weights, tokens):
    blocks, _, size = x.shape
    part = tokens // 2
    return pl.pallas_call(
        functools.partial(project_kernel, half, gain_row, scale),
        out_shape=(
            jax.ShapeDtypeStruct((part, size), jnp.bfloat16),
            jax.ShapeDtypeStruct((2, part, size), jnp.bfloat16),
        ),
        in_specs=[vmem()] * 3,
        out_specs=(vmem(),) * 2,
        scratch_shapes=[pltpu.VMEM((part, blocks * size), jnp.bfloat16)],
        cost_estimate=pl.CostEstimate(
            flops=2 * part * blocks * size * 3 * size, bytes_accessed=8 << 20, transcendentals=0
        ),
        compiler_params=pltpu.CompilerParams(vmem_limit_bytes=PROJECT_VMEM),
        name="project",
    )(x, gain, weights)


def attend_kernel(at_ref, qa_ref, qb_ref, low_ref, a_ref, b_ref, high_ref, bias_ref, x_ref, out_ref, keys, values):
    width = GRID_W
    half, size = qa_ref.shape
    rows = 2 * half // width
    for i, ref in enumerate((low_ref, a_ref, b_ref, high_ref)):
        keys[i * half : (i + 1) * half] = ref[0]
        values[i * half : (i + 1) * half] = ref[1]
    row_start, last = at_ref[0], at_ref[1]
    factor = size ** (-0.5)
    for r in range(rows):
        grid_row = row_start + r
        first = jnp.clip(grid_row - HALO, 0, last)
        at = pl.multiple_of((first - row_start + HALO) * width, width)
        offset = first - grid_row + 7
        span = pl.ds(at, WINDOW_ROWS * width)
        source, inner = (qa_ref, r) if r < rows // 2 else (qb_ref, r - rows // 2)
        query = source[inner * width : (inner + 1) * width, :]
        scores = lax.dot_general(
            query, keys[span, :], (((1,), (1,)), ((), ())), preferred_element_type=jnp.float32
        )
        parts = [
            scores[:, 2 * p * width : 2 * (p + 1) * width] * factor + bias_ref[offset + 2 * p]
            for p in range(WINDOW_ROWS // 2)
        ]
        top = functools.reduce(jnp.maximum, parts)
        top = jnp.max(top, axis=1, keepdims=True)
        parts = [jnp.exp(part - top) for part in parts]
        total = jnp.sum(functools.reduce(jnp.add, parts), axis=1, keepdims=True)
        inverse = 1.0 / total
        weight = jnp.concatenate([(part * inverse).astype(jnp.bfloat16) for part in parts], axis=1)
        attended = jnp.dot(weight, values[span, :], preferred_element_type=jnp.float32)
        here = slice(r * width, (r + 1) * width)
        out_ref[here, :] = (x_ref[here, :].astype(jnp.float32) + attended).astype(jnp.bfloat16)


def attend(at, queries, low, own, high, bias, x):
    tokens, size = x.shape
    long = tokens + 2 * HALO * GRID_W
    return pl.pallas_call(
        attend_kernel,
        out_shape=jax.ShapeDtypeStruct((tokens, size), jnp.bfloat16),
        in_specs=[pl.BlockSpec(memory_space=pltpu.SMEM)] + [vmem()] * 8,
        out_specs=vmem(),
        scratch_shapes=[pltpu.VMEM((long, size), jnp.bfloat16)] * 2,
        cost_estimate=pl.CostEstimate(
            flops=4 * tokens * size * WINDOW_ROWS * GRID_W, bytes_accessed=2 << 20, transcendentals=tokens * 512
        ),
        compiler_params=pltpu.CompilerParams(vmem_limit_bytes=ATTEND_VMEM),
        name="attend",
    )(at, *queries, low, *own, high, bias, x)


def layer(x, gathered, gain_row, scale, gains, weights, bias, at):
    tokens = x.shape[0]
    count = lax.axis_size("sp")
    forward = [(i, i + 1) for i in range(count - 1)]
    backward = [(target, source) for source, target in forward]
    query_high, own_high = project(1, gain_row, scale, gathered, gains, weights, tokens)
    low = lax.ppermute(own_high, "sp", forward)
    query_low, own_low = project(0, gain_row, scale, gathered, gains, weights, tokens)
    high = lax.ppermute(own_low, "sp", backward)
    return attend(at, (query_low, query_high), low, (own_low, own_high), high, bias, x)


def replicated(weights):
    block = jnp.concatenate(weights, 1)
    return jnp.broadcast_to(block[None], (lax.axis_size("sp"), *block.shape))


def spread(blocks):
    got = lax.all_to_all(blocks, "sp", 0, 0, tiled=True)
    return got.reshape(-1, blocks.shape[-1])


def body(
    stream,
    gain_first,
    query_first,
    key_first,
    value_first,
    offset_first,
    gain_second,
    query_second,
    key_second,
    value_second,
    offset_second,
):
    tokens, size = stream.shape
    rows = tokens // GRID_W
    first_set = spread(replicated((query_first, key_first, value_first)))
    second_blocks = replicated((query_second, key_second, value_second))
    bias_first, bias_second = biases(offset_first, offset_second)
    start = lax.axis_index("sp") * rows
    total_rows = rows * lax.axis_size("sp")
    at = jnp.stack([start, jnp.int32(total_rows - WINDOW_ROWS)]).astype(jnp.int32)

    gains = jnp.pad(jnp.stack([gain_first, gain_second]), ((0, 14), (0, 0)))
    sent = (jnp.concatenate([stream, gains]).astype(jnp.float32) * SCALE_FIRST).astype(jnp.float16)
    held = lax.all_gather(sent, "tp", axis=0, tiled=False).astype(jnp.bfloat16)
    gains = held[:, tokens:]
    middle = layer(stream, held, 0, SCALE_FIRST, gains, first_set, bias_first, at)
    middle, second_blocks = lax.optimization_barrier((middle, second_blocks))
    second_set = spread(second_blocks)
    sent = (middle.astype(jnp.float32) * SCALE_SECOND).astype(jnp.float16)
    again = lax.all_gather(sent, "tp", axis=0, tiled=False).astype(jnp.bfloat16)
    return layer(middle, again, 1, SCALE_SECOND, gains, second_set, bias_second, at)


def solution(mesh):
    placed = (
        P("sp", "tp"),
        P("tp"),
        P("sp", "tp"),
        P("sp", "tp"),
        P("sp", "tp"),
        P("tp", None, None),
        P("tp"),
        P("sp", "tp"),
        P("sp", "tp"),
        P("sp", "tp"),
        P("tp", None, None),
    )
    return jax.shard_map(body, mesh=mesh, in_specs=placed, out_specs=P("sp", "tp"), check_vma=False)
```

```python
import functools

import jax
import jax.numpy as jnp
from jax import lax
from jax.experimental import pallas as pl
from jax.experimental.pallas import tpu as pltpu
from jax.sharding import PartitionSpec as P


GRID_W = 64
EPSILON = 1e-06
SCALE_FIRST = 2.0**13
SCALE_SECOND = 2.0**6
WINDOW_ROWS = 8
HALO = 4
MASKED = -1e30
PROJECT_VMEM = 24 << 20
ATTEND_VMEM = 12 << 20


def vmem():
    return pl.BlockSpec(memory_space=pltpu.VMEM)


def bias_kernel(table_ref, out_ref):
    width = GRID_W
    col = lax.broadcasted_iota(jnp.int32, (width, 2 * width), 0)
    key = lax.broadcasted_iota(jnp.int32, (width, 2 * width), 1) % width
    start = jnp.clip(col - 8, 0, width - 16)
    inside = (key >= start) & (key < start + 16)
    low = jnp.pad(table_ref[0], ((0, 1), (0, 2 * width - table_ref.shape[2])))
    both = low + pltpu.roll(pltpu.roll(low, 15, 0), width, 1)
    for m in range(14):
        row = jnp.broadcast_to(both[m : m + 1, :], (width, 2 * width))
        turned = pltpu.roll(row, 2 * width - 15, 1, stride=1, stride_axis=0)
        out_ref[m] = jnp.where(inside, turned, MASKED)


def bias_of(table):
    return pl.pallas_call(
        bias_kernel,
        out_shape=jax.ShapeDtypeStruct((14, GRID_W, 2 * GRID_W), jnp.float32),
        in_specs=[vmem()],
        out_specs=vmem(),
        compiler_params=pltpu.CompilerParams(vmem_limit_bytes=ATTEND_VMEM),
        name="bias",
    )(table)


def project_kernel(half, gain_row, scale, x_ref, gain_ref, w_ref, q_ref, kv_ref, normed):
    blocks, _, size = x_ref.shape
    tokens = q_ref.shape[0]
    rows = slice(half * tokens, (half + 1) * tokens)
    total = jnp.zeros((tokens, size), jnp.float32)
    for f in range(blocks):
        part = x_ref[f, rows, :].astype(jnp.float32)
        total = total + part * part
    mean = jnp.sum(total, axis=1, keepdims=True) * (1.0 / (blocks * size * scale * scale))
    rate = lax.rsqrt(mean + EPSILON) * (1.0 / scale)
    for f in range(blocks):
        part = x_ref[f, rows, :].astype(jnp.float32)
        gain = gain_ref[f, gain_row : gain_row + 1, :].astype(jnp.float32) * (1.0 / SCALE_FIRST)
        normed[:, f * size : (f + 1) * size] = (part * rate * gain).astype(jnp.bfloat16)
    out = jnp.dot(normed[...], w_ref[...], preferred_element_type=jnp.float32).astype(jnp.bfloat16)
    q_ref[...] = out[:, :size]
    kv_ref[0] = out[:, size : 2 * size]
    kv_ref[1] = out[:, 2 * size :]


def project(half, gain_row, scale, x, gain, weights, tokens):
    blocks, _, size = x.shape
    part = tokens // 2
    return pl.pallas_call(
        functools.partial(project_kernel, half, gain_row, scale),
        out_shape=(
            jax.ShapeDtypeStruct((part, size), jnp.bfloat16),
            jax.ShapeDtypeStruct((2, part, size), jnp.bfloat16),
        ),
        in_specs=[vmem()] * 3,
        out_specs=(vmem(),) * 2,
        scratch_shapes=[pltpu.VMEM((part, blocks * size), jnp.bfloat16)],
        cost_estimate=pl.CostEstimate(
            flops=2 * part * blocks * size * 3 * size, bytes_accessed=8 << 20, transcendentals=0
        ),
        compiler_params=pltpu.CompilerParams(vmem_limit_bytes=PROJECT_VMEM),
        name="project",
    )(x, gain, weights)


def attend_kernel(at_ref, qa_ref, qb_ref, low_ref, a_ref, b_ref, high_ref, bias_ref, x_ref, out_ref, keys, values):
    width = GRID_W
    half, size = qa_ref.shape
    rows = 2 * half // width
    for i, ref in enumerate((low_ref, a_ref, b_ref, high_ref)):
        keys[i * half : (i + 1) * half] = ref[0]
        values[i * half : (i + 1) * half] = ref[1]
    row_start, last = at_ref[0], at_ref[1]
    factor = size ** (-0.5)
    for r in range(rows):
        grid_row = row_start + r
        first = jnp.clip(grid_row - HALO, 0, last)
        at = pl.multiple_of((first - row_start + HALO) * width, width)
        offset = first - grid_row + 7
        span = pl.ds(at, WINDOW_ROWS * width)
        source, inner = (qa_ref, r) if r < rows // 2 else (qb_ref, r - rows // 2)
        query = source[inner * width : (inner + 1) * width, :]
        scores = lax.dot_general(
            query, keys[span, :], (((1,), (1,)), ((), ())), preferred_element_type=jnp.float32
        )
        parts = [
            scores[:, 2 * p * width : 2 * (p + 1) * width] * factor + bias_ref[offset + 2 * p]
            for p in range(WINDOW_ROWS // 2)
        ]
        top = functools.reduce(jnp.maximum, parts)
        top = jnp.max(top, axis=1, keepdims=True)
        parts = [jnp.exp(part - top) for part in parts]
        total = jnp.sum(functools.reduce(jnp.add, parts), axis=1, keepdims=True)
        inverse = 1.0 / total
        weight = jnp.concatenate([(part * inverse).astype(jnp.bfloat16) for part in parts], axis=1)
        attended = jnp.dot(weight, values[span, :], preferred_element_type=jnp.float32)
        here = slice(r * width, (r + 1) * width)
        out_ref[here, :] = (x_ref[here, :].astype(jnp.float32) + attended).astype(jnp.bfloat16)


def attend(at, queries, low, own, high, bias, x):
    tokens, size = x.shape
    long = tokens + 2 * HALO * GRID_W
    return pl.pallas_call(
        attend_kernel,
        out_shape=jax.ShapeDtypeStruct((tokens, size), jnp.bfloat16),
        in_specs=[pl.BlockSpec(memory_space=pltpu.SMEM)] + [vmem()] * 8,
        out_specs=vmem(),
        scratch_shapes=[pltpu.VMEM((long, size), jnp.bfloat16)] * 2,
        cost_estimate=pl.CostEstimate(
            flops=4 * tokens * size * WINDOW_ROWS * GRID_W, bytes_accessed=2 << 20, transcendentals=tokens * 512
        ),
        compiler_params=pltpu.CompilerParams(vmem_limit_bytes=ATTEND_VMEM),
        name="attend",
    )(at, *queries, low, *own, high, bias, x)


def layer(x, gathered, gain_row, scale, gains, weights, table, at, following=None):
    tokens = x.shape[0]
    count = lax.axis_size("sp")
    forward = [(i, i + 1) for i in range(count - 1)]
    backward = [(target, source) for source, target in forward]
    query_high, own_high = project(1, gain_row, scale, gathered, gains, weights, tokens)
    low = lax.ppermute(own_high, "sp", forward)
    query_low, own_low = project(0, gain_row, scale, gathered, gains, weights, tokens)
    high = lax.ppermute(own_low, "sp", backward)
    if following is not None:
        query_low, following = lax.optimization_barrier((query_low, following))
        following = spread(following)
    bias = bias_of(table)
    out = attend(at, (query_low, query_high), low, (own_low, own_high), high, bias, x)
    return out, following


def replicated(weights):
    block = jnp.concatenate(weights, 1)
    return jnp.broadcast_to(block[None], (lax.axis_size("sp"), *block.shape))


def spread(blocks):
    got = lax.all_to_all(blocks, "sp", 0, 0, tiled=True)
    return got.reshape(-1, blocks.shape[-1])


def body(
    stream,
    gain_first,
    query_first,
    key_first,
    value_first,
    offset_first,
    gain_second,
    query_second,
    key_second,
    value_second,
    offset_second,
):
    tokens, _ = stream.shape
    rows = tokens // GRID_W
    first_set = spread(replicated((query_first, key_first, value_first)))
    second_blocks = replicated((query_second, key_second, value_second))
    start = lax.axis_index("sp") * rows
    total_rows = rows * lax.axis_size("sp")
    at = jnp.stack([start, jnp.int32(total_rows - WINDOW_ROWS)]).astype(jnp.int32)

    gains = jnp.pad(jnp.stack([gain_first, gain_second]), ((0, 6), (0, 0)))
    sent = (jnp.concatenate([stream, gains]).astype(jnp.float32) * SCALE_FIRST).astype(jnp.float16)
    held = lax.all_gather(sent, "tp", axis=0, tiled=False)
    held, first_set = lax.optimization_barrier((held, first_set))
    held = held.astype(jnp.bfloat16)
    gains = held[:, tokens:]
    middle, second_set = layer(
        stream, held, 0, SCALE_FIRST, gains, first_set, offset_first, at, second_blocks
    )
    sent = (middle.astype(jnp.float32) * SCALE_SECOND).astype(jnp.float16)
    again = lax.all_gather(sent, "tp", axis=0, tiled=False)
    again, second_set = lax.optimization_barrier((again, second_set))
    again = again.astype(jnp.bfloat16)
    return layer(middle, again, 1, SCALE_SECOND, gains, second_set, offset_second, at)[0]


def solution(mesh):
    placed = (
        P("sp", "tp"),
        P("tp"),
        P("sp", "tp"),
        P("sp", "tp"),
        P("sp", "tp"),
        P("tp", None, None),
        P("tp"),
        P("sp", "tp"),
        P("sp", "tp"),
        P("sp", "tp"),
        P("tp", None, None),
    )
    return jax.shard_map(body, mesh=mesh, in_specs=placed, out_specs=P("sp", "tp"), check_vma=False)
```

```python
import functools

import jax
import jax.numpy as jnp
from jax import lax
from jax.experimental import pallas as pl
from jax.experimental.pallas import tpu as pltpu
from jax.sharding import PartitionSpec as P


GRID_W = 64
EPSILON = 1e-06
SCALE_FIRST = 2.0**13
SCALE_SECOND = 2.0**6
WINDOW_ROWS = 8
HALO = 4
MASKED = -1e30
PROJECT_VMEM = 63_000_000
ATTEND_VMEM = 12 << 20
COPIES_VMEM = 66_000_000


def vmem():
    return pl.BlockSpec(memory_space=pltpu.VMEM)


def bias_kernel(table_ref, out_ref):
    width = GRID_W
    col = lax.broadcasted_iota(jnp.int32, (width, 2 * width), 0)
    key = lax.broadcasted_iota(jnp.int32, (width, 2 * width), 1) % width
    start = jnp.clip(col - 8, 0, width - 16)
    inside = (key >= start) & (key < start + 16)
    low = jnp.pad(table_ref[0], ((0, 1), (0, 2 * width - table_ref.shape[2])))
    both = low + pltpu.roll(pltpu.roll(low, 15, 0), width, 1)
    for m in range(14):
        row = jnp.broadcast_to(both[m : m + 1, :], (width, 2 * width))
        turned = pltpu.roll(row, 2 * width - 15, 1, stride=1, stride_axis=0)
        out_ref[m] = jnp.where(inside, turned, MASKED)


def bias_of(table):
    return pl.pallas_call(
        bias_kernel,
        out_shape=jax.ShapeDtypeStruct((14, GRID_W, 2 * GRID_W), jnp.float32),
        in_specs=[vmem()],
        out_specs=vmem(),
        compiler_params=pltpu.CompilerParams(vmem_limit_bytes=ATTEND_VMEM),
        name="bias",
    )(table)


def core_of_chip():
    return lax.rem(lax.axis_index("tp"), 2)


def project_kernel(gain_row, scale, x_hbm, gain_ref, w_ref, q_ref, a_ref, b_ref, x_ref, normed, sems):
    blocks, tokens, size = x_ref.shape
    half = tokens // 2
    core = core_of_chip()
    copies = [
        pltpu.make_async_copy(x_hbm.at[f, pl.ds(0, tokens)], x_ref.at[f], sems.at[f])
        for f in range(blocks)
    ]
    for copy in copies:
        copy.start()
    total = jnp.zeros((tokens, size), jnp.float32)
    for f in range(blocks):
        copies[f].wait()
        part = x_ref[f].astype(jnp.float32)
        total = total + part * part
    mean = jnp.sum(total, axis=1, keepdims=True) * (1.0 / (blocks * size * scale * scale))
    rate = lax.rsqrt(mean + EPSILON) * (1.0 / scale)
    for f in range(blocks):
        part = x_ref[f].astype(jnp.float32)
        gain = gain_ref[f, gain_row : gain_row + 1, :].astype(jnp.float32) * (1.0 / SCALE_FIRST)
        normed[:, f * size : (f + 1) * size] = (part * rate * gain).astype(jnp.bfloat16)
    for out_ref, number in ((a_ref, 1 - core), (b_ref, core)):
        rows = pl.ds(pl.multiple_of(number * half, half), half)
        out = jnp.dot(normed[rows, :], w_ref[...], preferred_element_type=jnp.float32)
        out = out.astype(jnp.bfloat16)
        q_ref[rows, :] = out[:, :size]
        out_ref[0] = out[:, size : 2 * size]
        out_ref[1] = out[:, 2 * size :]


def project(gain_row, scale, x, gain, weights, tokens):
    blocks, _, size = x.shape
    kv = jax.ShapeDtypeStruct((2, tokens // 2, size), jnp.bfloat16)
    return pl.pallas_call(
        functools.partial(project_kernel, gain_row, scale),
        out_shape=(jax.ShapeDtypeStruct((tokens, size), jnp.bfloat16), kv, kv),
        in_specs=[pl.BlockSpec(memory_space=pltpu.HBM), vmem(), vmem()],
        out_specs=(vmem(),) * 3,
        scratch_shapes=[
            pltpu.VMEM((blocks, tokens, size), jnp.bfloat16),
            pltpu.VMEM((tokens, blocks * size), jnp.bfloat16),
            pltpu.SemaphoreType.DMA((blocks,)),
        ],
        cost_estimate=pl.CostEstimate(
            flops=2 * tokens * blocks * size * 3 * size, bytes_accessed=8 << 20, transcendentals=0
        ),
        compiler_params=pltpu.CompilerParams(vmem_limit_bytes=PROJECT_VMEM),
        name="project",
    )(x, gain, weights)


def attend_kernel(last, q_ref, a_in, a_own, b_own, b_in, bias_ref, x_ref, out_ref, keys, values):
    width = GRID_W
    tokens, size = q_ref.shape
    half = tokens // 2
    rows = tokens // width
    core = core_of_chip()
    row_start = lax.axis_index("sp") * rows
    placed = (
        (a_in, core * 3),
        (a_own, 2 - core),
        (b_own, 1 + core),
        (b_in, (1 - core) * 3),
    )
    for ref, number in placed:
        span = pl.ds(pl.multiple_of(number * half, half), half)
        keys[span, :] = ref[0]
        values[span, :] = ref[1]
    factor = size ** (-0.5)
    spans, scored = [], []
    for r in range(rows):
        grid_row = row_start + r
        first = jnp.clip(grid_row - HALO, 0, last)
        at = pl.multiple_of((first - row_start + HALO) * width, width)
        offset = first - grid_row + 7
        spans.append(pl.ds(at, WINDOW_ROWS * width))
        scores = lax.dot_general(
            q_ref[r * width : (r + 1) * width, :],
            keys[spans[r], :],
            (((1,), (1,)), ((), ())),
            preferred_element_type=jnp.float32,
        )
        scored.append(
            [
                scores[:, 2 * p * width : 2 * (p + 1) * width] * factor + bias_ref[offset + 2 * p]
                for p in range(WINDOW_ROWS // 2)
            ]
        )
    weights = []
    for parts in scored:
        top = jnp.max(functools.reduce(jnp.maximum, parts), axis=1, keepdims=True)
        parts = [jnp.exp(part - top) for part in parts]
        total = jnp.sum(functools.reduce(jnp.add, parts), axis=1, keepdims=True)
        inverse = 1.0 / total
        weights.append(jnp.concatenate([(part * inverse).astype(jnp.bfloat16) for part in parts], 1))
    for r in range(rows):
        attended = jnp.dot(weights[r], values[spans[r], :], preferred_element_type=jnp.float32)
        here = slice(r * width, (r + 1) * width)
        out_ref[here, :] = (x_ref[here, :].astype(jnp.float32) + attended).astype(jnp.bfloat16)


def attend(last, query, a_in, a_own, b_own, b_in, bias, x):
    tokens, size = x.shape
    return pl.pallas_call(
        functools.partial(attend_kernel, last),
        out_shape=jax.ShapeDtypeStruct((tokens, size), jnp.bfloat16),
        in_specs=[vmem()] * 7,
        out_specs=vmem(),
        scratch_shapes=[pltpu.VMEM((2 * tokens, size), jnp.bfloat16)] * 2,
        cost_estimate=pl.CostEstimate(
            flops=4 * tokens * size * WINDOW_ROWS * GRID_W, bytes_accessed=2 << 20, transcendentals=tokens * 512
        ),
        compiler_params=pltpu.CompilerParams(vmem_limit_bytes=ATTEND_VMEM),
        name="attend",
    )(query, a_in, a_own, b_own, b_in, bias, x)


def halo_pairs(first):
    count, across = lax.axis_size("sp"), lax.axis_size("tp")
    pairs = []
    for s in range(count):
        for t in range(across):
            target = s + 1 if (t % 2 == 0) == first else s - 1
            if 0 <= target < count:
                pairs.append((s * across + t, target * across + t))
    return pairs


def layer(x, gathered, gain_row, scale, gains, weights, table, following=None):
    tokens = x.shape[0]
    last = lax.axis_size("sp") * tokens // GRID_W - WINDOW_ROWS
    query, a_own, b_own = project(gain_row, scale, gathered, gains, weights, tokens)
    a_in = lax.ppermute(a_own, ("sp", "tp"), halo_pairs(True))
    b_in = lax.ppermute(b_own, ("sp", "tp"), halo_pairs(False))
    if following is not None:
        query, *following = lax.optimization_barrier((query, *following))
        following = spread(following)
    bias = bias_of(table)
    out = attend(last, query, a_in, a_own, b_own, b_in, bias, x)
    return out, following


def copies_kernel(first_ref, second_ref, third_ref, out_ref, block, sems):
    size = first_ref.shape[1]
    for i, ref in enumerate((first_ref, second_ref, third_ref)):
        block[:, i * size : (i + 1) * size] = ref[...]
    copies = [pltpu.make_async_copy(block, out_ref.at[i], sems.at[i]) for i in range(out_ref.shape[0])]
    for copy in copies:
        copy.start()
    for copy in copies:
        copy.wait()


def spread(weights):
    rows, size = weights[0].shape
    count = lax.axis_size("sp")
    blocks = pl.pallas_call(
        copies_kernel,
        out_shape=jax.ShapeDtypeStruct((count, rows, 3 * size), jnp.bfloat16),
        in_specs=[vmem()] * 3,
        out_specs=pl.BlockSpec(memory_space=pltpu.HBM),
        scratch_shapes=[pltpu.VMEM((rows, 3 * size), jnp.bfloat16), pltpu.SemaphoreType.DMA((count,))],
        compiler_params=pltpu.CompilerParams(vmem_limit_bytes=COPIES_VMEM),
        name="copies",
    )(*weights)
    return lax.all_to_all(blocks, "sp", 0, 0, tiled=True).reshape(-1, 3 * size)


def body(
    stream,
    gain_first,
    query_first,
    key_first,
    value_first,
    offset_first,
    gain_second,
    query_second,
    key_second,
    value_second,
    offset_second,
):
    tokens, _ = stream.shape
    first_set = spread((query_first, key_first, value_first))
    gains = jnp.pad(jnp.stack([gain_first, gain_second]), ((0, 6), (0, 0)))
    sent = (jnp.concatenate([stream, gains]).astype(jnp.float32) * SCALE_FIRST).astype(jnp.float16)
    held = lax.all_gather(sent, "tp", axis=0, tiled=False)
    gains = held[:, tokens:].astype(jnp.bfloat16)
    held = held.astype(jnp.bfloat16)
    middle, second_set = layer(
        stream,
        held,
        0,
        SCALE_FIRST,
        gains,
        first_set,
        offset_first,
        (query_second, key_second, value_second),
    )
    sent = (middle.astype(jnp.float32) * SCALE_SECOND).astype(jnp.float16)
    again = lax.all_gather(sent, "tp", axis=0, tiled=False).astype(jnp.bfloat16)
    return layer(middle, again, 1, SCALE_SECOND, gains, second_set, offset_second)[0]


def solution(mesh):
    placed = (
        P("sp", "tp"),
        P("tp"),
        P("sp", "tp"),
        P("sp", "tp"),
        P("sp", "tp"),
        P("tp", None, None),
        P("tp"),
        P("sp", "tp"),
        P("sp", "tp"),
        P("sp", "tp"),
        P("tp", None, None),
    )
    return jax.shard_map(body, mesh=mesh, in_specs=placed, out_specs=P("sp", "tp"), check_vma=False)
```

```python
import functools

import jax
import jax.numpy as jnp
from jax import lax
from jax.experimental import pallas as pl
from jax.experimental.pallas import tpu as pltpu
from jax.sharding import PartitionSpec as P


GRID_W = 64
EPSILON = 1e-06
SCALE_FIRST = 2.0**13
SCALE_SECOND = 2.0**6
WINDOW_ROWS = 8
HALO = 4
MASKED = -1e30
PROJECT_VMEM = 24 << 20
ATTEND_VMEM = 12 << 20
COPIES_VMEM = (66_000_000, 2 << 20)


def vmem():
    return pl.BlockSpec(memory_space=pltpu.VMEM)


def bias_kernel(table_ref, out_ref):
    width = GRID_W
    col = lax.broadcasted_iota(jnp.int32, (width, 2 * width), 0)
    key = lax.broadcasted_iota(jnp.int32, (width, 2 * width), 1) % width
    start = jnp.clip(col - 8, 0, width - 16)
    inside = (key >= start) & (key < start + 16)
    low = jnp.pad(table_ref[0], ((0, 1), (0, 2 * width - table_ref.shape[2])))
    both = low + pltpu.roll(pltpu.roll(low, 15, 0), width, 1)
    for m in range(14):
        row = jnp.broadcast_to(both[m : m + 1, :], (width, 2 * width))
        turned = pltpu.roll(row, 2 * width - 15, 1, stride=1, stride_axis=0)
        out_ref[m] = jnp.where(inside, turned, MASKED)


def bias_of(table):
    return pl.pallas_call(
        bias_kernel,
        out_shape=jax.ShapeDtypeStruct((14, GRID_W, 2 * GRID_W), jnp.float32),
        in_specs=[vmem()],
        out_specs=vmem(),
        compiler_params=pltpu.CompilerParams(vmem_limit_bytes=ATTEND_VMEM),
        name="bias",
    )(table)


def core_of_chip():
    return lax.rem(lax.axis_index("tp"), 2)


def project_kernel(gain_row, scale, x_ref, gain_ref, w_ref, q_ref, a_ref, b_ref, normed):
    blocks, _, size = x_ref.shape
    tokens = q_ref.shape[0]
    half = tokens // 2
    core = core_of_chip()
    total = jnp.zeros((tokens, size), jnp.float32)
    for f in range(blocks):
        part = x_ref[f, :tokens, :].astype(jnp.float32)
        total = total + part * part
    mean = jnp.sum(total, axis=1, keepdims=True) * (1.0 / (blocks * size * scale * scale))
    rate = lax.rsqrt(mean + EPSILON) * (1.0 / scale)
    for f in range(blocks):
        part = x_ref[f, :tokens, :].astype(jnp.float32)
        gain = gain_ref[f, gain_row : gain_row + 1, :].astype(jnp.float32) * (1.0 / SCALE_FIRST)
        normed[:, f * size : (f + 1) * size] = (part * rate * gain).astype(jnp.bfloat16)
    for out_ref, number in ((a_ref, 1 - core), (b_ref, core)):
        rows = pl.ds(pl.multiple_of(number * half, half), half)
        out = jnp.dot(normed[rows, :], w_ref[...], preferred_element_type=jnp.float32)
        out = out.astype(jnp.bfloat16)
        q_ref[rows, :] = out[:, :size]
        out_ref[0] = out[:, size : 2 * size]
        out_ref[1] = out[:, 2 * size :]


def project(gain_row, scale, x, gain, weights, tokens):
    blocks, _, size = x.shape
    kv = jax.ShapeDtypeStruct((2, tokens // 2, size), jnp.bfloat16)
    return pl.pallas_call(
        functools.partial(project_kernel, gain_row, scale),
        out_shape=(jax.ShapeDtypeStruct((tokens, size), jnp.bfloat16), kv, kv),
        in_specs=[vmem()] * 3,
        out_specs=(vmem(),) * 3,
        scratch_shapes=[pltpu.VMEM((tokens, blocks * size), jnp.bfloat16)],
        cost_estimate=pl.CostEstimate(
            flops=2 * tokens * blocks * size * 3 * size, bytes_accessed=8 << 20, transcendentals=0
        ),
        compiler_params=pltpu.CompilerParams(vmem_limit_bytes=PROJECT_VMEM),
        name="project",
    )(x, gain, weights)


def attend_kernel(last, q_ref, a_in, a_own, b_own, b_in, bias_ref, x_ref, out_ref, keys, values):
    width = GRID_W
    tokens, size = q_ref.shape
    half = tokens // 2
    rows = tokens // width
    core = core_of_chip()
    row_start = lax.axis_index("sp") * rows
    placed = (
        (a_in, core * 3),
        (a_own, 2 - core),
        (b_own, 1 + core),
        (b_in, (1 - core) * 3),
    )
    for ref, number in placed:
        span = pl.ds(pl.multiple_of(number * half, half), half)
        keys[span, :] = ref[0]
        values[span, :] = ref[1]
    factor = size ** (-0.5)
    spans, scored = [], []
    for r in range(rows):
        grid_row = row_start + r
        first = jnp.clip(grid_row - HALO, 0, last)
        at = pl.multiple_of((first - row_start + HALO) * width, width)
        offset = first - grid_row + 7
        spans.append(pl.ds(at, WINDOW_ROWS * width))
        scores = lax.dot_general(
            q_ref[r * width : (r + 1) * width, :],
            keys[spans[r], :],
            (((1,), (1,)), ((), ())),
            preferred_element_type=jnp.float32,
        )
        scored.append(
            [
                scores[:, 2 * p * width : 2 * (p + 1) * width] * factor + bias_ref[offset + 2 * p]
                for p in range(WINDOW_ROWS // 2)
            ]
        )
    weights = []
    for parts in scored:
        top = jnp.max(functools.reduce(jnp.maximum, parts), axis=1, keepdims=True)
        parts = [jnp.exp(part - top) for part in parts]
        total = jnp.sum(functools.reduce(jnp.add, parts), axis=1, keepdims=True)
        inverse = 1.0 / total
        weights.append(jnp.concatenate([(part * inverse).astype(jnp.bfloat16) for part in parts], 1))
    for r in range(rows):
        attended = jnp.dot(weights[r], values[spans[r], :], preferred_element_type=jnp.float32)
        here = slice(r * width, (r + 1) * width)
        out_ref[here, :] = (x_ref[here, :].astype(jnp.float32) + attended).astype(jnp.bfloat16)


def attend(last, query, a_in, a_own, b_own, b_in, bias, x):
    tokens, size = x.shape
    return pl.pallas_call(
        functools.partial(attend_kernel, last),
        out_shape=jax.ShapeDtypeStruct((tokens, size), jnp.bfloat16),
        in_specs=[vmem()] * 7,
        out_specs=vmem(),
        scratch_shapes=[pltpu.VMEM((2 * tokens, size), jnp.bfloat16)] * 2,
        cost_estimate=pl.CostEstimate(
            flops=4 * tokens * size * WINDOW_ROWS * GRID_W, bytes_accessed=2 << 20, transcendentals=tokens * 512
        ),
        compiler_params=pltpu.CompilerParams(vmem_limit_bytes=ATTEND_VMEM),
        name="attend",
    )(query, a_in, a_own, b_own, b_in, bias, x)


def halo_pairs(first):
    count, across = lax.axis_size("sp"), lax.axis_size("tp")
    pairs = []
    for s in range(count):
        for t in range(across):
            target = s + 1 if (t % 2 == 0) == first else s - 1
            if 0 <= target < count:
                pairs.append((s * across + t, target * across + t))
    return pairs


def layer(x, gathered, gain_row, scale, gains, weights, table, following=None):
    tokens = x.shape[0]
    last = lax.axis_size("sp") * tokens // GRID_W - WINDOW_ROWS
    query, a_own, b_own = project(gain_row, scale, gathered, gains, weights, tokens)
    a_in = lax.ppermute(a_own, ("sp", "tp"), halo_pairs(True))
    b_in = lax.ppermute(b_own, ("sp", "tp"), halo_pairs(False))
    if following is not None:
        query, following = lax.optimization_barrier((query, following))
        following = spread(following)
    bias = bias_of(table)
    out = attend(last, query, a_in, a_own, b_own, b_in, bias, x)
    return out, following


def copies_kernel(first_ref, second_ref, third_ref, out_ref, block, sems):
    size = first_ref.shape[1]
    for i, ref in enumerate((first_ref, second_ref, third_ref)):
        block[:, i * size : (i + 1) * size] = ref[...]
    copies = [pltpu.make_async_copy(block, out_ref.at[i], sems.at[i]) for i in range(out_ref.shape[0])]
    for copy in copies:
        copy.start()
    for copy in copies:
        copy.wait()


def replicated(weights, grant):
    rows, size = weights[0].shape
    count = lax.axis_size("sp")
    return pl.pallas_call(
        copies_kernel,
        out_shape=jax.ShapeDtypeStruct((count, rows, 3 * size), jnp.bfloat16),
        in_specs=[vmem()] * 3,
        out_specs=pl.BlockSpec(memory_space=pltpu.HBM),
        scratch_shapes=[pltpu.VMEM((rows, 3 * size), jnp.bfloat16), pltpu.SemaphoreType.DMA((count,))],
        compiler_params=pltpu.CompilerParams(vmem_limit_bytes=grant),
        name="copies",
    )(*weights)


def spread(blocks):
    return lax.all_to_all(blocks, "sp", 0, 0, tiled=True).reshape(-1, blocks.shape[2])


def body(
    stream,
    gain_first,
    query_first,
    key_first,
    value_first,
    offset_first,
    gain_second,
    query_second,
    key_second,
    value_second,
    offset_second,
):
    tokens, _ = stream.shape
    first_blocks = replicated((query_first, key_first, value_first), COPIES_VMEM[0])
    first_blocks, *second = lax.optimization_barrier(
        (first_blocks, query_second, key_second, value_second)
    )
    second_blocks = replicated(second, COPIES_VMEM[1])
    first_set = spread(first_blocks)
    gains = jnp.pad(jnp.stack([gain_first, gain_second]), ((0, 6), (0, 0)))
    sent = (jnp.concatenate([stream, gains]).astype(jnp.float32) * SCALE_FIRST).astype(jnp.float16)
    sent, second_blocks = lax.optimization_barrier((sent, second_blocks))
    held = lax.all_gather(sent, "tp", axis=0, tiled=False)
    gains = held[:, tokens:].astype(jnp.bfloat16)
    held = held.astype(jnp.bfloat16)
    middle, second_set = layer(
        stream,
        held,
        0,
        SCALE_FIRST,
        gains,
        first_set,
        offset_first,
        second_blocks,
    )
    sent = (middle.astype(jnp.float32) * SCALE_SECOND).astype(jnp.float16)
    again = lax.all_gather(sent, "tp", axis=0, tiled=False).astype(jnp.bfloat16)
    return layer(middle, again, 1, SCALE_SECOND, gains, second_set, offset_second)[0]


def solution(mesh):
    placed = (
        P("sp", "tp"),
        P("tp"),
        P("sp", "tp"),
        P("sp", "tp"),
        P("sp", "tp"),
        P("tp", None, None),
        P("tp"),
        P("sp", "tp"),
        P("sp", "tp"),
        P("sp", "tp"),
        P("tp", None, None),
    )
    return jax.shard_map(body, mesh=mesh, in_specs=placed, out_specs=P("sp", "tp"), check_vma=False)
```

```python
import functools

import jax
import jax.numpy as jnp
from jax import lax
from jax.experimental import pallas as pl
from jax.experimental.pallas import tpu as pltpu
from jax.sharding import PartitionSpec as P


GRID_W = 64
EPSILON = 1e-06
SCALE_FIRST = 2.0**13
SCALE_SECOND = 2.0**6
WINDOW_ROWS = 8
HALO = 4
MASKED = -1e30
PROJECT_VMEM = 24 << 20
ATTEND_VMEM = 12 << 20
COPIES_VMEM = 66_000_000
BIAS_VMEM = (64_000_000, 12 << 20)


def vmem():
    return pl.BlockSpec(memory_space=pltpu.VMEM)


def bias_kernel(table_ref, out_ref):
    width = GRID_W
    col = lax.broadcasted_iota(jnp.int32, (width, 2 * width), 0)
    key = lax.broadcasted_iota(jnp.int32, (width, 2 * width), 1) % width
    start = jnp.clip(col - 8, 0, width - 16)
    inside = (key >= start) & (key < start + 16)
    low = jnp.pad(table_ref[0], ((0, 1), (0, 2 * width - table_ref.shape[2])))
    both = low + pltpu.roll(pltpu.roll(low, 15, 0), width, 1)
    for m in range(14):
        row = jnp.broadcast_to(both[m : m + 1, :], (width, 2 * width))
        turned = pltpu.roll(row, 2 * width - 15, 1, stride=1, stride_axis=0)
        out_ref[m] = jnp.where(inside, turned, MASKED)


def bias_of(table, grant):
    return pl.pallas_call(
        bias_kernel,
        out_shape=jax.ShapeDtypeStruct((14, GRID_W, 2 * GRID_W), jnp.float32),
        in_specs=[vmem()],
        out_specs=vmem(),
        compiler_params=pltpu.CompilerParams(vmem_limit_bytes=grant),
        name="bias",
    )(table)


def core_of_chip():
    return lax.rem(lax.axis_index("tp"), 2)


def project_kernel(gain_row, scale, x_ref, gain_ref, w_ref, q_ref, a_ref, b_ref, normed):
    blocks, _, size = x_ref.shape
    tokens = q_ref.shape[0]
    half = tokens // 2
    core = core_of_chip()
    total = jnp.zeros((tokens, size), jnp.float32)
    for f in range(blocks):
        part = x_ref[f, :tokens, :].astype(jnp.float32)
        total = total + part * part
    mean = jnp.sum(total, axis=1, keepdims=True) * (1.0 / (blocks * size * scale * scale))
    rate = lax.rsqrt(mean + EPSILON) * (1.0 / scale)
    for f in range(blocks):
        part = x_ref[f, :tokens, :].astype(jnp.float32)
        gain = gain_ref[f, gain_row : gain_row + 1, :].astype(jnp.float32) * (1.0 / SCALE_FIRST)
        normed[:, f * size : (f + 1) * size] = (part * rate * gain).astype(jnp.bfloat16)
    outs = []
    for number in range(2):
        rows = slice(number * half, (number + 1) * half)
        out = jnp.dot(normed[rows, :], w_ref[...], preferred_element_type=jnp.float32)
        out = out.astype(jnp.bfloat16)
        q_ref[rows, :] = out[:, :size]
        outs.append(out[:, size:])
    for out_ref, turn in ((a_ref, core), (b_ref, 1 - core)):
        out = jnp.where(turn == 0, outs[1], outs[0])
        out_ref[0] = out[:, :size]
        out_ref[1] = out[:, size:]


def project(gain_row, scale, x, gain, weights, tokens):
    blocks, _, size = x.shape
    kv = jax.ShapeDtypeStruct((2, tokens // 2, size), jnp.bfloat16)
    return pl.pallas_call(
        functools.partial(project_kernel, gain_row, scale),
        out_shape=(jax.ShapeDtypeStruct((tokens, size), jnp.bfloat16), kv, kv),
        in_specs=[vmem()] * 3,
        out_specs=(vmem(),) * 3,
        scratch_shapes=[pltpu.VMEM((tokens, blocks * size), jnp.bfloat16)],
        cost_estimate=pl.CostEstimate(
            flops=2 * tokens * blocks * size * 3 * size, bytes_accessed=8 << 20, transcendentals=0
        ),
        compiler_params=pltpu.CompilerParams(vmem_limit_bytes=PROJECT_VMEM),
        name="project",
    )(x, gain, weights)


def attend_kernel(last, q_ref, a_in, a_own, b_own, b_in, bias_ref, x_ref, out_ref, keys, values):
    width = GRID_W
    tokens, size = q_ref.shape
    half = tokens // 2
    rows = tokens // width
    core = core_of_chip()
    row_start = lax.axis_index("sp") * rows
    placed = (
        (a_in, core * 3),
        (a_own, 2 - core),
        (b_own, 1 + core),
        (b_in, (1 - core) * 3),
    )
    for ref, number in placed:
        span = pl.ds(pl.multiple_of(number * half, half), half)
        keys[span, :] = ref[0]
        values[span, :] = ref[1]
    factor = size ** (-0.5)
    spans, scored = [], []
    for r in range(rows):
        grid_row = row_start + r
        first = jnp.clip(grid_row - HALO, 0, last)
        at = pl.multiple_of((first - row_start + HALO) * width, width)
        offset = first - grid_row + 7
        spans.append(pl.ds(at, WINDOW_ROWS * width))
        scores = lax.dot_general(
            q_ref[r * width : (r + 1) * width, :],
            keys[spans[r], :],
            (((1,), (1,)), ((), ())),
            preferred_element_type=jnp.float32,
        )
        scored.append(
            [
                scores[:, 2 * p * width : 2 * (p + 1) * width] * factor + bias_ref[offset + 2 * p]
                for p in range(WINDOW_ROWS // 2)
            ]
        )
    weights = []
    for parts in scored:
        top = jnp.max(functools.reduce(jnp.maximum, parts), axis=1, keepdims=True)
        parts = [jnp.exp(part - top) for part in parts]
        total = jnp.sum(functools.reduce(jnp.add, parts), axis=1, keepdims=True)
        inverse = 1.0 / total
        weights.append(jnp.concatenate([(part * inverse).astype(jnp.bfloat16) for part in parts], 1))
    for r in range(rows):
        attended = jnp.dot(weights[r], values[spans[r], :], preferred_element_type=jnp.float32)
        here = slice(r * width, (r + 1) * width)
        out_ref[here, :] = (x_ref[here, :].astype(jnp.float32) + attended).astype(jnp.bfloat16)


def attend(last, query, a_in, a_own, b_own, b_in, bias, x):
    tokens, size = x.shape
    return pl.pallas_call(
        functools.partial(attend_kernel, last),
        out_shape=jax.ShapeDtypeStruct((tokens, size), jnp.bfloat16),
        in_specs=[vmem()] * 7,
        out_specs=vmem(),
        scratch_shapes=[pltpu.VMEM((2 * tokens, size), jnp.bfloat16)] * 2,
        cost_estimate=pl.CostEstimate(
            flops=4 * tokens * size * WINDOW_ROWS * GRID_W, bytes_accessed=2 << 20, transcendentals=tokens * 512
        ),
        compiler_params=pltpu.CompilerParams(vmem_limit_bytes=ATTEND_VMEM),
        name="attend",
    )(query, a_in, a_own, b_own, b_in, bias, x)


def halo_pairs(first):
    count, across = lax.axis_size("sp"), lax.axis_size("tp")
    pairs = []
    for s in range(count):
        for t in range(across):
            target = s + 1 if (t % 2 == 0) == first else s - 1
            if 0 <= target < count:
                pairs.append((s * across + t, target * across + t))
    return pairs


def layer(x, gathered, gain_row, scale, gains, weights, table, following=None):
    tokens = x.shape[0]
    last = lax.axis_size("sp") * tokens // GRID_W - WINDOW_ROWS
    query, a_own, b_own = project(gain_row, scale, gathered, gains, weights, tokens)
    a_in = lax.ppermute(a_own, ("sp", "tp"), halo_pairs(True))
    b_in = lax.ppermute(b_own, ("sp", "tp"), halo_pairs(False))
    if following is not None:
        query, following = lax.optimization_barrier((query, following))
        following = spread(following)
    bias = bias_of(table, BIAS_VMEM[gain_row])
    out = attend(last, query, a_in, a_own, b_own, b_in, bias, x)
    return out, following


def copies_kernel(first_ref, second_ref, third_ref, out_ref, block, sems):
    size = first_ref.shape[1]
    for i, ref in enumerate((first_ref, second_ref, third_ref)):
        block[:, i * size : (i + 1) * size] = ref[...]
    copies = [pltpu.make_async_copy(block, out_ref.at[i], sems.at[i]) for i in range(out_ref.shape[0])]
    for copy in copies:
        copy.start()
    for copy in copies:
        copy.wait()


def replicated(weights):
    rows, size = weights[0].shape
    count = lax.axis_size("sp")
    return pl.pallas_call(
        copies_kernel,
        out_shape=jax.ShapeDtypeStruct((count, rows, 3 * size), jnp.bfloat16),
        in_specs=[vmem()] * 3,
        out_specs=pl.BlockSpec(memory_space=pltpu.HBM),
        scratch_shapes=[pltpu.VMEM((rows, 3 * size), jnp.bfloat16), pltpu.SemaphoreType.DMA((count,))],
        compiler_params=pltpu.CompilerParams(vmem_limit_bytes=COPIES_VMEM),
        name="copies",
    )(*weights)


def spread(blocks):
    return lax.all_to_all(blocks, "sp", 0, 0, tiled=True).reshape(-1, blocks.shape[2])


def body(
    stream,
    gain_first,
    query_first,
    key_first,
    value_first,
    offset_first,
    gain_second,
    query_second,
    key_second,
    value_second,
    offset_second,
):
    tokens, _ = stream.shape
    first_blocks = replicated((query_first, key_first, value_first))
    first_blocks, *second = lax.optimization_barrier(
        (first_blocks, query_second, key_second, value_second)
    )
    second_blocks = jnp.concatenate(second, 1)
    second_blocks = jnp.broadcast_to(second_blocks[None], first_blocks.shape)
    first_set = spread(first_blocks)
    gains = jnp.pad(jnp.stack([gain_first, gain_second]), ((0, 6), (0, 0)))
    sent = (jnp.concatenate([stream, gains]).astype(jnp.float32) * SCALE_FIRST).astype(jnp.float16)
    sent, second_blocks = lax.optimization_barrier((sent, second_blocks))
    held = lax.all_gather(sent, "tp", axis=0, tiled=False)
    gains = held[:, tokens:].astype(jnp.bfloat16)
    held = held.astype(jnp.bfloat16)
    middle, second_set = layer(
        stream,
        held,
        0,
        SCALE_FIRST,
        gains,
        first_set,
        offset_first,
        second_blocks,
    )
    sent = (middle.astype(jnp.float32) * SCALE_SECOND).astype(jnp.float16)
    again = lax.all_gather(sent, "tp", axis=0, tiled=False).astype(jnp.bfloat16)
    return layer(middle, again, 1, SCALE_SECOND, gains, second_set, offset_second)[0]


def solution(mesh):
    placed = (
        P("sp", "tp"),
        P("tp"),
        P("sp", "tp"),
        P("sp", "tp"),
        P("sp", "tp"),
        P("tp", None, None),
        P("tp"),
        P("sp", "tp"),
        P("sp", "tp"),
        P("sp", "tp"),
        P("tp", None, None),
    )
    return jax.shard_map(body, mesh=mesh, in_specs=placed, out_specs=P("sp", "tp"), check_vma=False)
```

```python
import functools

import jax
import jax.numpy as jnp
from jax import lax
from jax.experimental import pallas as pl
from jax.experimental.pallas import tpu as pltpu
from jax.sharding import PartitionSpec as P


GRID_W = 64
EPSILON = 1e-06
SCALE_FIRST = 2.0**13
SCALE_SECOND = 2.0**6
WINDOW_ROWS = 8
HALO = 4
MASKED = -1e30
PROJECT_VMEM = 24 << 20
COPIES_VMEM = 66_000_000
ATTEND_VMEM = 12 << 20


def vmem():
    return pl.BlockSpec(memory_space=pltpu.VMEM)


def fill_bias(table_ref, bias_ref):
    width = GRID_W
    col = lax.broadcasted_iota(jnp.int32, (width, 2 * width), 0)
    key = lax.broadcasted_iota(jnp.int32, (width, 2 * width), 1) % width
    start = jnp.clip(col - 8, 0, width - 16)
    inside = (key >= start) & (key < start + 16)
    low = jnp.pad(table_ref[0], ((0, 1), (0, 2 * width - table_ref.shape[2])))
    both = low + pltpu.roll(pltpu.roll(low, 15, 0), width, 1)
    for m in range(14):
        row = jnp.broadcast_to(both[m : m + 1, :], (width, 2 * width))
        turned = pltpu.roll(row, 2 * width - 15, 1, stride=1, stride_axis=0)
        bias_ref[m] = jnp.where(inside, turned, MASKED)


def core_of_chip():
    return lax.rem(lax.axis_index("tp"), 2)


def project_kernel(gain_row, scale, x_hbm, gain_hbm, w_ref, q_ref, a_ref, b_ref, x_ref, gain_ref, normed, sems):
    blocks, tokens, size = x_ref.shape
    half = tokens // 2
    core = core_of_chip()
    copies = [
        pltpu.make_async_copy(x_hbm.at[f, pl.ds(0, tokens)], x_ref.at[f], sems.at[f])
        for f in range(blocks)
    ]
    rows = gain_hbm.shape[1] - tokens
    gains = pltpu.make_async_copy(gain_hbm.at[:, pl.ds(tokens, rows)], gain_ref, sems.at[blocks])
    for copy in copies:
        copy.start()
    gains.start()
    total = jnp.zeros((tokens, size), jnp.float32)
    for f in range(blocks):
        copies[f].wait()
        part = x_ref[f].astype(jnp.float32)
        total = total + part * part
    mean = jnp.sum(total, axis=1, keepdims=True) * (1.0 / (blocks * size * scale * scale))
    rate = lax.rsqrt(mean + EPSILON) * (1.0 / scale)
    gains.wait()
    for f in range(blocks):
        part = x_ref[f].astype(jnp.float32)
        gain = gain_ref[f, gain_row : gain_row + 1, :].astype(jnp.float32) * (1.0 / SCALE_FIRST)
        normed[:, f * size : (f + 1) * size] = (part * rate * gain).astype(jnp.bfloat16)
    outs = []
    for number in range(2):
        rows = slice(number * half, (number + 1) * half)
        out = jnp.dot(normed[rows, :], w_ref[...], preferred_element_type=jnp.float32)
        out = out.astype(jnp.bfloat16)
        q_ref[rows, :] = out[:, :size]
        outs.append(out[:, size:])
    for out_ref, turn in ((a_ref, core), (b_ref, 1 - core)):
        out = jnp.where(turn == 0, outs[1], outs[0])
        out_ref[0] = out[:, :size]
        out_ref[1] = out[:, size:]


def project(gain_row, scale, x, held, weights, tokens):
    blocks, _, size = x.shape
    kv = jax.ShapeDtypeStruct((2, tokens // 2, size), jnp.bfloat16)
    hbm = pl.BlockSpec(memory_space=pltpu.HBM)
    return pl.pallas_call(
        functools.partial(project_kernel, gain_row, scale),
        out_shape=(jax.ShapeDtypeStruct((tokens, size), jnp.bfloat16), kv, kv),
        in_specs=[hbm, hbm, vmem()],
        out_specs=(vmem(),) * 3,
        scratch_shapes=[
            pltpu.VMEM((blocks, tokens, size), jnp.bfloat16),
            pltpu.VMEM((blocks, held.shape[1] - tokens, size), jnp.bfloat16),
            pltpu.VMEM((tokens, blocks * size), jnp.bfloat16),
            pltpu.SemaphoreType.DMA((blocks + 1,)),
        ],
        cost_estimate=pl.CostEstimate(
            flops=2 * tokens * blocks * size * 3 * size, bytes_accessed=8 << 20, transcendentals=0
        ),
        compiler_params=pltpu.CompilerParams(vmem_limit_bytes=PROJECT_VMEM),
        name="project",
    )(x, held, weights)


def attend_kernel(last, q_ref, a_in, a_own, b_own, b_in, table_ref, x_ref, out_ref, keys, values, bias_ref):
    fill_bias(table_ref, bias_ref)
    width = GRID_W
    tokens, size = q_ref.shape
    half = tokens // 2
    rows = tokens // width
    core = core_of_chip()
    row_start = lax.axis_index("sp") * rows
    placed = (
        (a_in, core * 3),
        (a_own, 2 - core),
        (b_own, 1 + core),
        (b_in, (1 - core) * 3),
    )
    for ref, number in placed:
        span = pl.ds(pl.multiple_of(number * half, half), half)
        keys[span, :] = ref[0]
        values[span, :] = ref[1]
    factor = size ** (-0.5)
    spans, scored = [], []
    for r in range(rows):
        grid_row = row_start + r
        first = jnp.clip(grid_row - HALO, 0, last)
        at = pl.multiple_of((first - row_start + HALO) * width, width)
        offset = first - grid_row + 7
        spans.append(pl.ds(at, WINDOW_ROWS * width))
        scores = lax.dot_general(
            q_ref[r * width : (r + 1) * width, :],
            keys[spans[r], :],
            (((1,), (1,)), ((), ())),
            preferred_element_type=jnp.float32,
        )
        scored.append(
            [
                scores[:, 2 * p * width : 2 * (p + 1) * width] * factor + bias_ref[offset + 2 * p]
                for p in range(WINDOW_ROWS // 2)
            ]
        )
    weights = []
    for parts in scored:
        top = jnp.max(functools.reduce(jnp.maximum, parts), axis=1, keepdims=True)
        parts = [jnp.exp(part - top) for part in parts]
        total = jnp.sum(functools.reduce(jnp.add, parts), axis=1, keepdims=True)
        inverse = 1.0 / total
        weights.append(jnp.concatenate([(part * inverse).astype(jnp.bfloat16) for part in parts], 1))
    for r in range(rows):
        attended = jnp.dot(weights[r], values[spans[r], :], preferred_element_type=jnp.float32)
        here = slice(r * width, (r + 1) * width)
        out_ref[here, :] = (x_ref[here, :].astype(jnp.float32) + attended).astype(jnp.bfloat16)


def attend(last, query, a_in, a_own, b_own, b_in, table, x):
    tokens, size = x.shape
    return pl.pallas_call(
        functools.partial(attend_kernel, last),
        out_shape=jax.ShapeDtypeStruct((tokens, size), jnp.bfloat16),
        in_specs=[vmem()] * 7,
        out_specs=vmem(),
        scratch_shapes=[
            pltpu.VMEM((2 * tokens, size), jnp.bfloat16),
            pltpu.VMEM((2 * tokens, size), jnp.bfloat16),
            pltpu.VMEM((14, GRID_W, 2 * GRID_W), jnp.float32),
        ],
        cost_estimate=pl.CostEstimate(
            flops=4 * tokens * size * WINDOW_ROWS * GRID_W, bytes_accessed=2 << 20, transcendentals=tokens * 512
        ),
        compiler_params=pltpu.CompilerParams(vmem_limit_bytes=ATTEND_VMEM),
        name="attend",
    )(query, a_in, a_own, b_own, b_in, table, x)


def halo_pairs(first):
    count, across = lax.axis_size("sp"), lax.axis_size("tp")
    pairs = []
    for s in range(count):
        for t in range(across):
            target = s + 1 if (t % 2 == 0) == first else s - 1
            if 0 <= target < count:
                pairs.append((s * across + t, target * across + t))
    return pairs


def layer(x, gathered, gain_row, scale, held, weights, table, following=None):
    tokens = x.shape[0]
    last = lax.axis_size("sp") * tokens // GRID_W - WINDOW_ROWS
    query, a_own, b_own = project(gain_row, scale, gathered, held, weights, tokens)
    a_in = lax.ppermute(a_own, ("sp", "tp"), halo_pairs(True))
    b_in = lax.ppermute(b_own, ("sp", "tp"), halo_pairs(False))
    if following is not None:
        query, following = lax.optimization_barrier((query, following))
        following = spread(following)
    out = attend(last, query, a_in, a_own, b_own, b_in, table, x)
    return out, following


def copies_kernel(first_ref, second_ref, third_ref, out_ref, block, sems):
    size = first_ref.shape[1]
    for i, ref in enumerate((first_ref, second_ref, third_ref)):
        block[:, i * size : (i + 1) * size] = ref[...]
    copies = [pltpu.make_async_copy(block, out_ref.at[i], sems.at[i]) for i in range(out_ref.shape[0])]
    for copy in copies:
        copy.start()
    for copy in copies:
        copy.wait()


def replicated(weights):
    rows, size = weights[0].shape
    count = lax.axis_size("sp")
    return pl.pallas_call(
        copies_kernel,
        out_shape=jax.ShapeDtypeStruct((count, rows, 3 * size), jnp.bfloat16),
        in_specs=[vmem()] * 3,
        out_specs=pl.BlockSpec(memory_space=pltpu.HBM),
        scratch_shapes=[pltpu.VMEM((rows, 3 * size), jnp.bfloat16), pltpu.SemaphoreType.DMA((count,))],
        compiler_params=pltpu.CompilerParams(vmem_limit_bytes=COPIES_VMEM),
        name="copies",
    )(*weights)


def spread(blocks):
    return lax.all_to_all(blocks, "sp", 0, 0, tiled=True).reshape(-1, blocks.shape[2])


def body(
    stream,
    gain_first,
    query_first,
    key_first,
    value_first,
    offset_first,
    gain_second,
    query_second,
    key_second,
    value_second,
    offset_second,
):
    first_blocks = replicated((query_first, key_first, value_first))
    first_blocks, *second = lax.optimization_barrier(
        (first_blocks, query_second, key_second, value_second)
    )
    second_blocks = jnp.concatenate(second, 1)
    second_blocks = jnp.broadcast_to(second_blocks[None], first_blocks.shape)
    first_set = spread(first_blocks)
    gains = jnp.pad(jnp.stack([gain_first, gain_second]), ((0, 6), (0, 0)))
    sent = (jnp.concatenate([stream, gains]).astype(jnp.float32) * SCALE_FIRST).astype(jnp.float16)
    sent, second_blocks = lax.optimization_barrier((sent, second_blocks))
    held = lax.all_gather(sent, "tp", axis=0, tiled=False).astype(jnp.bfloat16)
    held = pltpu.with_memory_space_constraint(held, pltpu.HBM)
    middle, second_set = layer(
        stream,
        held,
        0,
        SCALE_FIRST,
        held,
        first_set,
        offset_first,
        second_blocks,
    )
    sent = (middle.astype(jnp.float32) * SCALE_SECOND).astype(jnp.float16)
    again = lax.all_gather(sent, "tp", axis=0, tiled=False).astype(jnp.bfloat16)
    again = pltpu.with_memory_space_constraint(again, pltpu.HBM)
    return layer(middle, again, 1, SCALE_SECOND, held, second_set, offset_second)[0]


def solution(mesh):
    placed = (
        P("sp", "tp"),
        P("tp"),
        P("sp", "tp"),
        P("sp", "tp"),
        P("sp", "tp"),
        P("tp", None, None),
        P("tp"),
        P("sp", "tp"),
        P("sp", "tp"),
        P("sp", "tp"),
        P("tp", None, None),
    )
    return jax.shard_map(body, mesh=mesh, in_specs=placed, out_specs=P("sp", "tp"), check_vma=False)
```

```python
import functools

import jax
import jax.numpy as jnp
from jax import lax
from jax.experimental import pallas as pl
from jax.experimental.pallas import tpu as pltpu
from jax.sharding import PartitionSpec as P


GRID_W = 64
EPSILON = 1e-06
SCALE_FIRST = 2.0**13
SCALE_SECOND = 2.0**6
WINDOW_ROWS = 8
HALO = 4
MASKED = -1e30
PROJECT_VMEM = 24 << 20
COPIES_VMEM = 66_000_000
NEAR_BLOCKS = 22
ATTEND_VMEM = 12 << 20


def vmem():
    return pl.BlockSpec(memory_space=pltpu.VMEM)


def fill_bias(table_ref, bias_ref):
    width = GRID_W
    col = lax.broadcasted_iota(jnp.int32, (width, 2 * width), 0)
    key = lax.broadcasted_iota(jnp.int32, (width, 2 * width), 1) % width
    start = jnp.clip(col - 8, 0, width - 16)
    inside = (key >= start) & (key < start + 16)
    low = jnp.pad(table_ref[0], ((0, 1), (0, 2 * width - table_ref.shape[2])))
    both = low + pltpu.roll(pltpu.roll(low, 15, 0), width, 1)
    for m in range(14):
        row = jnp.broadcast_to(both[m : m + 1, :], (width, 2 * width))
        turned = pltpu.roll(row, 2 * width - 15, 1, stride=1, stride_axis=0)
        bias_ref[m] = jnp.where(inside, turned, MASKED)


def core_of_chip():
    return lax.rem(lax.axis_index("tp"), 2)


def project_kernel(gain_row, scale, near, *refs):
    near_ref, refs = (refs[0], refs[1:]) if near else (None, refs)
    x_hbm, gain_hbm, w_in, q_ref, a_ref, b_ref, x_ref, gain_ref, normed, sems, *rest = refs
    far, tokens, size = x_ref.shape
    blocks = near + far
    half = tokens // 2
    core = core_of_chip()
    copies = [
        pltpu.make_async_copy(x_hbm.at[f, pl.ds(0, tokens)], x_ref.at[f], sems.at[f])
        for f in range(far)
    ]

    def block_of(f):
        return near_ref[f] if f < near else x_ref[f - near]

    rows = gain_hbm.shape[1] - tokens
    gains = pltpu.make_async_copy(gain_hbm.at[:, pl.ds(tokens, rows)], gain_ref, sems.at[blocks])
    for copy in copies:
        copy.start()
    gains.start()
    w_ref = w_in
    if rest:
        (w_ref,) = rest
        weights = pltpu.make_async_copy(w_in, w_ref, sems.at[blocks + 1])
        weights.start()
    total = jnp.zeros((tokens, size), jnp.float32)
    for f in range(blocks):
        if f >= near:
            copies[f - near].wait()
        part = block_of(f).astype(jnp.float32)
        total = total + part * part
    mean = jnp.sum(total, axis=1, keepdims=True) * (1.0 / (blocks * size * scale * scale))
    rate = lax.rsqrt(mean + EPSILON) * (1.0 / scale)
    gains.wait()
    for f in range(blocks):
        part = block_of(f).astype(jnp.float32)
        gain = gain_ref[f, gain_row : gain_row + 1, :].astype(jnp.float32) * (1.0 / SCALE_FIRST)
        normed[:, f * size : (f + 1) * size] = (part * rate * gain).astype(jnp.bfloat16)
    if rest:
        weights.wait()
    outs = []
    for number in range(2):
        rows = slice(number * half, (number + 1) * half)
        out = jnp.dot(normed[rows, :], w_ref[...], preferred_element_type=jnp.float32)
        out = out.astype(jnp.bfloat16)
        q_ref[rows, :] = out[:, :size]
        outs.append(out[:, size:])
    for out_ref, turn in ((a_ref, core), (b_ref, 1 - core)):
        out = jnp.where(turn == 0, outs[1], outs[0])
        out_ref[0] = out[:, :size]
        out_ref[1] = out[:, size:]


def project(gain_row, scale, x, held, weights, tokens):
    *nearer, x = x
    near = nearer[0].shape[0] if nearer else 0
    far, _, size = x.shape
    blocks = near + far
    kv = jax.ShapeDtypeStruct((2, tokens // 2, size), jnp.bfloat16)
    hbm = pl.BlockSpec(memory_space=pltpu.HBM)
    streamed = gain_row == 1
    return pl.pallas_call(
        functools.partial(project_kernel, gain_row, scale, near),
        out_shape=(jax.ShapeDtypeStruct((tokens, size), jnp.bfloat16), kv, kv),
        in_specs=[vmem()] * len(nearer) + [hbm, hbm, hbm if streamed else vmem()],
        out_specs=(vmem(),) * 3,
        scratch_shapes=[
            pltpu.VMEM((far, tokens, size), jnp.bfloat16),
            pltpu.VMEM((blocks, held.shape[1] - tokens, size), jnp.bfloat16),
            pltpu.VMEM((tokens, blocks * size), jnp.bfloat16),
            pltpu.SemaphoreType.DMA((blocks + 2,)),
        ]
        + [pltpu.VMEM(weights.shape, jnp.bfloat16)] * streamed,
        cost_estimate=pl.CostEstimate(
            flops=2 * tokens * blocks * size * 3 * size, bytes_accessed=8 << 20, transcendentals=0
        ),
        compiler_params=pltpu.CompilerParams(vmem_limit_bytes=PROJECT_VMEM),
        name="project",
    )(*nearer, x, held, weights)


def attend_kernel(last, q_ref, a_in, a_own, b_own, b_in, table_ref, x_ref, out_ref, keys, values, bias_ref):
    fill_bias(table_ref, bias_ref)
    width = GRID_W
    tokens, size = q_ref.shape
    half = tokens // 2
    rows = tokens // width
    core = core_of_chip()
    row_start = lax.axis_index("sp") * rows
    placed = (
        (a_in, core * 3),
        (a_own, 2 - core),
        (b_own, 1 + core),
        (b_in, (1 - core) * 3),
    )
    for ref, number in placed:
        span = pl.ds(pl.multiple_of(number * half, half), half)
        keys[span, :] = ref[0]
        values[span, :] = ref[1]
    factor = size ** (-0.5)
    spans, scored = [], []
    for r in range(rows):
        grid_row = row_start + r
        first = jnp.clip(grid_row - HALO, 0, last)
        at = pl.multiple_of((first - row_start + HALO) * width, width)
        offset = first - grid_row + 7
        spans.append(pl.ds(at, WINDOW_ROWS * width))
        scores = lax.dot_general(
            q_ref[r * width : (r + 1) * width, :],
            keys[spans[r], :],
            (((1,), (1,)), ((), ())),
            preferred_element_type=jnp.float32,
        )
        scored.append(
            [
                scores[:, 2 * p * width : 2 * (p + 1) * width] * factor + bias_ref[offset + 2 * p]
                for p in range(WINDOW_ROWS // 2)
            ]
        )
    weights = []
    for parts in scored:
        top = jnp.max(functools.reduce(jnp.maximum, parts), axis=1, keepdims=True)
        parts = [jnp.exp(part - top) for part in parts]
        total = jnp.sum(functools.reduce(jnp.add, parts), axis=1, keepdims=True)
        inverse = 1.0 / total
        weights.append(jnp.concatenate([(part * inverse).astype(jnp.bfloat16) for part in parts], 1))
    for r in range(rows):
        attended = jnp.dot(weights[r], values[spans[r], :], preferred_element_type=jnp.float32)
        here = slice(r * width, (r + 1) * width)
        out_ref[here, :] = (x_ref[here, :].astype(jnp.float32) + attended).astype(jnp.bfloat16)


def attend(last, query, a_in, a_own, b_own, b_in, table, x):
    tokens, size = x.shape
    return pl.pallas_call(
        functools.partial(attend_kernel, last),
        out_shape=jax.ShapeDtypeStruct((tokens, size), jnp.bfloat16),
        in_specs=[vmem()] * 7,
        out_specs=vmem(),
        scratch_shapes=[
            pltpu.VMEM((2 * tokens, size), jnp.bfloat16),
            pltpu.VMEM((2 * tokens, size), jnp.bfloat16),
            pltpu.VMEM((14, GRID_W, 2 * GRID_W), jnp.float32),
        ],
        cost_estimate=pl.CostEstimate(
            flops=4 * tokens * size * WINDOW_ROWS * GRID_W, bytes_accessed=2 << 20, transcendentals=tokens * 512
        ),
        compiler_params=pltpu.CompilerParams(vmem_limit_bytes=ATTEND_VMEM),
        name="attend",
    )(query, a_in, a_own, b_own, b_in, table, x)


def halo_pairs(first):
    count, across = lax.axis_size("sp"), lax.axis_size("tp")
    pairs = []
    for s in range(count):
        for t in range(across):
            target = s + 1 if (t % 2 == 0) == first else s - 1
            if 0 <= target < count:
                pairs.append((s * across + t, target * across + t))
    return pairs


def layer(x, gathered, gain_row, scale, held, weights, table, following=None):
    tokens = x.shape[0]
    last = lax.axis_size("sp") * tokens // GRID_W - WINDOW_ROWS
    query, a_own, b_own = project(gain_row, scale, gathered, held, weights, tokens)
    a_in = lax.ppermute(a_own, ("sp", "tp"), halo_pairs(True))
    b_in = lax.ppermute(b_own, ("sp", "tp"), halo_pairs(False))
    if following is not None:
        query, following = lax.optimization_barrier((query, following))
        following = pltpu.with_memory_space_constraint(spread(following), pltpu.HBM)
    out = attend(last, query, a_in, a_own, b_own, b_in, table, x)
    return out, following


def copies_kernel(first_ref, second_ref, third_ref, out_ref, block, sems):
    size = first_ref.shape[1]
    for i, ref in enumerate((first_ref, second_ref, third_ref)):
        block[:, i * size : (i + 1) * size] = ref[...]
    copies = [pltpu.make_async_copy(block, out_ref.at[i], sems.at[i]) for i in range(out_ref.shape[0])]
    for copy in copies:
        copy.start()
    for copy in copies:
        copy.wait()


def replicated(weights):
    rows, size = weights[0].shape
    count = lax.axis_size("sp")
    return pl.pallas_call(
        copies_kernel,
        out_shape=jax.ShapeDtypeStruct((count, rows, 3 * size), jnp.bfloat16),
        in_specs=[vmem()] * 3,
        out_specs=pl.BlockSpec(memory_space=pltpu.HBM),
        scratch_shapes=[pltpu.VMEM((rows, 3 * size), jnp.bfloat16), pltpu.SemaphoreType.DMA((count,))],
        compiler_params=pltpu.CompilerParams(vmem_limit_bytes=COPIES_VMEM),
        name="copies",
    )(*weights)


def spread(blocks):
    return lax.all_to_all(blocks, "sp", 0, 0, tiled=True).reshape(-1, blocks.shape[2])


def body(
    stream,
    gain_first,
    query_first,
    key_first,
    value_first,
    offset_first,
    gain_second,
    query_second,
    key_second,
    value_second,
    offset_second,
):
    first_blocks = replicated((query_first, key_first, value_first))
    first_blocks, *second = lax.optimization_barrier(
        (first_blocks, query_second, key_second, value_second)
    )
    second_blocks = jnp.concatenate(second, 1)
    second_blocks = jnp.broadcast_to(second_blocks[None], first_blocks.shape)
    first_set = spread(first_blocks)
    gains = jnp.pad(jnp.stack([gain_first, gain_second]), ((0, 6), (0, 0)))
    sent = (jnp.concatenate([stream, gains]).astype(jnp.float32) * SCALE_FIRST).astype(jnp.float16)
    sent, second_blocks = lax.optimization_barrier((sent, second_blocks))
    held = lax.all_gather(sent, "tp", axis=0, tiled=False).astype(jnp.bfloat16)
    held = pltpu.with_memory_space_constraint(held, pltpu.HBM)
    middle, second_set = layer(
        stream,
        (held,),
        0,
        SCALE_FIRST,
        held,
        first_set,
        offset_first,
        second_blocks,
    )
    sent = (middle.astype(jnp.float32) * SCALE_SECOND).astype(jnp.float16)
    again = lax.all_gather(sent, "tp", axis=0, tiled=False)
    near = again[:NEAR_BLOCKS].astype(jnp.bfloat16)
    far = again[NEAR_BLOCKS:].astype(jnp.bfloat16)
    again = (near, pltpu.with_memory_space_constraint(far, pltpu.HBM))
    return layer(middle, again, 1, SCALE_SECOND, held, second_set, offset_second)[0]


def solution(mesh):
    placed = (
        P("sp", "tp"),
        P("tp"),
        P("sp", "tp"),
        P("sp", "tp"),
        P("sp", "tp"),
        P("tp", None, None),
        P("tp"),
        P("sp", "tp"),
        P("sp", "tp"),
        P("sp", "tp"),
        P("tp", None, None),
    )
    return jax.shard_map(body, mesh=mesh, in_specs=placed, out_specs=P("sp", "tp"), check_vma=False)
```

```python
import functools

import jax
import jax.numpy as jnp
from jax import lax
from jax.experimental import pallas as pl
from jax.experimental.pallas import tpu as pltpu
from jax.sharding import PartitionSpec as P


GRID_W = 64
EPSILON = 1e-06
SCALE_FIRST = 2.0**13
SCALE_SECOND = 2.0**6
WINDOW_ROWS = 8
HALO = 4
MASKED = -1e30
PROJECT_VMEM = 24 << 20
COPIES_VMEM = 66_000_000
NEAR_BLOCKS = 22
GROUP = 10
ATTEND_VMEM = 12 << 20


def vmem():
    return pl.BlockSpec(memory_space=pltpu.VMEM)


def fill_bias(table_ref, bias_ref):
    width = GRID_W
    col = lax.broadcasted_iota(jnp.int32, (width, 2 * width), 0)
    key = lax.broadcasted_iota(jnp.int32, (width, 2 * width), 1) % width
    start = jnp.clip(col - 8, 0, width - 16)
    inside = (key >= start) & (key < start + 16)
    low = jnp.pad(table_ref[0], ((0, 1), (0, 2 * width - table_ref.shape[2])))
    both = low + pltpu.roll(pltpu.roll(low, 15, 0), width, 1)
    for m in range(14):
        row = jnp.broadcast_to(both[m : m + 1, :], (width, 2 * width))
        turned = pltpu.roll(row, 2 * width - 15, 1, stride=1, stride_axis=0)
        bias_ref[m] = jnp.where(inside, turned, MASKED)


def core_of_chip():
    return lax.rem(lax.axis_index("tp"), 2)


def project_kernel(gain_row, scale, near, *refs):
    near_ref, refs = (refs[0], refs[1:]) if near else (None, refs)
    x_hbm, gain_hbm, w_in, q_ref, a_ref, b_ref, x_ref, gain_ref, normed, sems, *rest = refs
    far, tokens, size = x_ref.shape
    blocks = near + far
    half = tokens // 2
    core = core_of_chip()
    copies = [
        pltpu.make_async_copy(x_hbm.at[f, pl.ds(0, tokens)], x_ref.at[f], sems.at[f])
        for f in range(far)
    ]

    def block_of(f):
        return near_ref[f] if f < near else x_ref[f - near]

    rows = gain_hbm.shape[1] - tokens
    gains = pltpu.make_async_copy(gain_hbm.at[:, pl.ds(tokens, rows)], gain_ref, sems.at[blocks])
    for copy in copies:
        copy.start()
    gains.start()
    w_ref = w_in
    if rest:
        (w_ref,) = rest
        weights = pltpu.make_async_copy(w_in, w_ref, sems.at[blocks + 1])
        weights.start()
    total = jnp.zeros((tokens, size), jnp.float32)
    for f in range(blocks):
        if f >= near and (f - near) % GROUP == 0:
            for copy in copies[f - near : f - near + GROUP]:
                copy.wait()
        part = block_of(f).astype(jnp.float32)
        total = total + part * part
    mean = jnp.sum(total, axis=1, keepdims=True) * (1.0 / (blocks * size * scale * scale))
    rate = lax.rsqrt(mean + EPSILON) * (1.0 / scale)
    gains.wait()
    for f in range(blocks):
        part = block_of(f).astype(jnp.float32)
        gain = gain_ref[f, gain_row : gain_row + 1, :].astype(jnp.float32) * (1.0 / SCALE_FIRST)
        normed[:, f * size : (f + 1) * size] = (part * rate * gain).astype(jnp.bfloat16)
    if rest:
        weights.wait()
    outs = []
    for number in range(2):
        rows = slice(number * half, (number + 1) * half)
        out = jnp.dot(normed[rows, :], w_ref[...], preferred_element_type=jnp.float32)
        out = out.astype(jnp.bfloat16)
        q_ref[rows, :] = out[:, :size]
        outs.append(out[:, size:])
    for out_ref, turn in ((a_ref, core), (b_ref, 1 - core)):
        out = jnp.where(turn == 0, outs[1], outs[0])
        out_ref[0] = out[:, :size]
        out_ref[1] = out[:, size:]


def project(gain_row, scale, x, held, weights, tokens):
    *nearer, x = x
    near = nearer[0].shape[0] if nearer else 0
    far, _, size = x.shape
    blocks = near + far
    kv = jax.ShapeDtypeStruct((2, tokens // 2, size), jnp.bfloat16)
    hbm = pl.BlockSpec(memory_space=pltpu.HBM)
    streamed = gain_row == 1
    return pl.pallas_call(
        functools.partial(project_kernel, gain_row, scale, near),
        out_shape=(jax.ShapeDtypeStruct((tokens, size), jnp.bfloat16), kv, kv),
        in_specs=[vmem()] * len(nearer) + [hbm, hbm, hbm if streamed else vmem()],
        out_specs=(vmem(),) * 3,
        scratch_shapes=[
            pltpu.VMEM((far, tokens, size), jnp.bfloat16),
            pltpu.VMEM((blocks, held.shape[1] - tokens, size), jnp.bfloat16),
            pltpu.VMEM((tokens, blocks * size), jnp.bfloat16),
            pltpu.SemaphoreType.DMA((blocks + 2,)),
        ]
        + [pltpu.VMEM(weights.shape, jnp.bfloat16)] * streamed,
        cost_estimate=pl.CostEstimate(
            flops=2 * tokens * blocks * size * 3 * size, bytes_accessed=8 << 20, transcendentals=0
        ),
        compiler_params=pltpu.CompilerParams(vmem_limit_bytes=PROJECT_VMEM),
        name="project",
    )(*nearer, x, held, weights)


def attend_kernel(last, q_ref, a_in, a_own, b_own, b_in, table_ref, x_ref, out_ref, keys, values, bias_ref):
    fill_bias(table_ref, bias_ref)
    width = GRID_W
    tokens, size = q_ref.shape
    half = tokens // 2
    rows = tokens // width
    core = core_of_chip()
    row_start = lax.axis_index("sp") * rows
    placed = (
        (a_in, core * 3),
        (a_own, 2 - core),
        (b_own, 1 + core),
        (b_in, (1 - core) * 3),
    )
    for ref, number in placed:
        span = pl.ds(pl.multiple_of(number * half, half), half)
        keys[span, :] = ref[0]
        values[span, :] = ref[1]
    factor = size ** (-0.5)
    spans, scored = [], []
    for r in range(rows):
        grid_row = row_start + r
        first = jnp.clip(grid_row - HALO, 0, last)
        at = pl.multiple_of((first - row_start + HALO) * width, width)
        offset = first - grid_row + 7
        spans.append(pl.ds(at, WINDOW_ROWS * width))
        scores = lax.dot_general(
            q_ref[r * width : (r + 1) * width, :],
            keys[spans[r], :],
            (((1,), (1,)), ((), ())),
            preferred_element_type=jnp.float32,
        )
        scored.append(
            [
                scores[:, 2 * p * width : 2 * (p + 1) * width] * factor + bias_ref[offset + 2 * p]
                for p in range(WINDOW_ROWS // 2)
            ]
        )
    weights = []
    for parts in scored:
        top = jnp.max(functools.reduce(jnp.maximum, parts), axis=1, keepdims=True)
        parts = [jnp.exp(part - top) for part in parts]
        total = jnp.sum(functools.reduce(jnp.add, parts), axis=1, keepdims=True)
        inverse = 1.0 / total
        weights.append(jnp.concatenate([(part * inverse).astype(jnp.bfloat16) for part in parts], 1))
    for r in range(rows):
        attended = jnp.dot(weights[r], values[spans[r], :], preferred_element_type=jnp.float32)
        here = slice(r * width, (r + 1) * width)
        out_ref[here, :] = (x_ref[here, :].astype(jnp.float32) + attended).astype(jnp.bfloat16)


def attend(last, query, a_in, a_own, b_own, b_in, table, x):
    tokens, size = x.shape
    return pl.pallas_call(
        functools.partial(attend_kernel, last),
        out_shape=jax.ShapeDtypeStruct((tokens, size), jnp.bfloat16),
        in_specs=[vmem()] * 7,
        out_specs=vmem(),
        scratch_shapes=[
            pltpu.VMEM((2 * tokens, size), jnp.bfloat16),
            pltpu.VMEM((2 * tokens, size), jnp.bfloat16),
            pltpu.VMEM((14, GRID_W, 2 * GRID_W), jnp.float32),
        ],
        cost_estimate=pl.CostEstimate(
            flops=4 * tokens * size * WINDOW_ROWS * GRID_W, bytes_accessed=2 << 20, transcendentals=tokens * 512
        ),
        compiler_params=pltpu.CompilerParams(vmem_limit_bytes=ATTEND_VMEM),
        name="attend",
    )(query, a_in, a_own, b_own, b_in, table, x)


def halo_pairs(first):
    count, across = lax.axis_size("sp"), lax.axis_size("tp")
    pairs = []
    for s in range(count):
        for t in range(across):
            target = s + 1 if (t % 2 == 0) == first else s - 1
            if 0 <= target < count:
                pairs.append((s * across + t, target * across + t))
    return pairs


def layer(x, gathered, gain_row, scale, held, weights, table, following=None):
    tokens = x.shape[0]
    last = lax.axis_size("sp") * tokens // GRID_W - WINDOW_ROWS
    query, a_own, b_own = project(gain_row, scale, gathered, held, weights, tokens)
    a_in = lax.ppermute(a_own, ("sp", "tp"), halo_pairs(True))
    b_in = lax.ppermute(b_own, ("sp", "tp"), halo_pairs(False))
    if following is not None:
        query, following = lax.optimization_barrier((query, following))
        following = pltpu.with_memory_space_constraint(spread(following), pltpu.HBM)
    out = attend(last, query, a_in, a_own, b_own, b_in, table, x)
    return out, following


def copies_kernel(first_ref, second_ref, third_ref, out_ref, block, sems):
    size = first_ref.shape[1]
    for i, ref in enumerate((first_ref, second_ref, third_ref)):
        block[:, i * size : (i + 1) * size] = ref[...]
    copies = [pltpu.make_async_copy(block, out_ref.at[i], sems.at[i]) for i in range(out_ref.shape[0])]
    for copy in copies:
        copy.start()
    for copy in copies:
        copy.wait()


def replicated(weights):
    rows, size = weights[0].shape
    count = lax.axis_size("sp")
    return pl.pallas_call(
        copies_kernel,
        out_shape=jax.ShapeDtypeStruct((count, rows, 3 * size), jnp.bfloat16),
        in_specs=[vmem()] * 3,
        out_specs=pl.BlockSpec(memory_space=pltpu.HBM),
        scratch_shapes=[pltpu.VMEM((rows, 3 * size), jnp.bfloat16), pltpu.SemaphoreType.DMA((count,))],
        compiler_params=pltpu.CompilerParams(vmem_limit_bytes=COPIES_VMEM),
        name="copies",
    )(*weights)


def spread(blocks):
    return lax.all_to_all(blocks, "sp", 0, 0, tiled=True).reshape(-1, blocks.shape[2])


def body(
    stream,
    gain_first,
    query_first,
    key_first,
    value_first,
    offset_first,
    gain_second,
    query_second,
    key_second,
    value_second,
    offset_second,
):
    first_blocks = replicated((query_first, key_first, value_first))
    first_blocks, *second = lax.optimization_barrier(
        (first_blocks, query_second, key_second, value_second)
    )
    second_blocks = jnp.concatenate(second, 1)
    second_blocks = jnp.broadcast_to(second_blocks[None], first_blocks.shape)
    first_set = spread(first_blocks)
    gains = jnp.pad(jnp.stack([gain_first, gain_second]), ((0, 6), (0, 0)))
    sent = (jnp.concatenate([stream, gains]).astype(jnp.float32) * SCALE_FIRST).astype(jnp.float16)
    sent, second_blocks = lax.optimization_barrier((sent, second_blocks))
    held = lax.all_gather(sent, "tp", axis=0, tiled=False).astype(jnp.bfloat16)
    held = pltpu.with_memory_space_constraint(held, pltpu.HBM)
    middle, second_set = layer(
        stream,
        (held,),
        0,
        SCALE_FIRST,
        held,
        first_set,
        offset_first,
        second_blocks,
    )
    sent = (middle.astype(jnp.float32) * SCALE_SECOND).astype(jnp.float16)
    again = lax.all_gather(sent, "tp", axis=0, tiled=False)
    near = again[:NEAR_BLOCKS].astype(jnp.bfloat16)
    far = again[NEAR_BLOCKS:].astype(jnp.bfloat16)
    again = (near, pltpu.with_memory_space_constraint(far, pltpu.HBM))
    return layer(middle, again, 1, SCALE_SECOND, held, second_set, offset_second)[0]


def solution(mesh):
    placed = (
        P("sp", "tp"),
        P("tp"),
        P("sp", "tp"),
        P("sp", "tp"),
        P("sp", "tp"),
        P("tp", None, None),
        P("tp"),
        P("sp", "tp"),
        P("sp", "tp"),
        P("sp", "tp"),
        P("tp", None, None),
    )
    return jax.shard_map(body, mesh=mesh, in_specs=placed, out_specs=P("sp", "tp"), check_vma=False)
```
